32 devices in a mesh: sp: 8 (over z, core), tp: 4 (over y, x).
Axes of the slice: x: 2, y: 2, z: 4, core: 2. Of those that a mesh axis runs over, the one named last changes fastest.
Arguments:
- layer_input: bfloat16 [8, 1024, 2048], P(None, 'sp', 'tp'), may hold values from -6 to 6
- w_key: bfloat16 [2048, 2048], P(None, 'tp'), may hold values from -0.125 to 0.125
- w_value: bfloat16 [2048, 2048], P(None, 'tp'), may hold values from -0.125 to 0.125
- w_gates: bfloat16 [2, 2048, 16], replicated, may hold values from -0.125 to 0.125
- decay_rate: float32 [16], P('tp'), may hold values from 0 to 1, as said below
- beta_bias: float32 [16], P('tp'), may hold values from -5.5 to -3
- log_decay_extra: float32 [8, 16, 1024], P(None, 'tp', 'sp'), may hold values from -2 to 0, as said below
- new_query: bfloat16 [8, 2048], P(None, 'tp'), may hold values from -6 to 6
- read_gain: float32 [128], replicated, may hold values from 0.1 to 1.9
Outputs:
- state_cache: bfloat16 [1024, 2048], P('sp', 'tp')
- first_read: bfloat16 [8, 2048], P(None, 'tp')
The draws below stay inside these ranges and needn't reach their ends.
Inputs may be any that keep to these rules, and one draw needn't show every extreme that they name: `decay_rate`: a positive rate for each head. `log_decay_extra`: additions that are never positive.
All inputs are finite; a program needn't handle non-finite values.
Results may differ from the reference program's by a relative error of at most 0.0052.
Values may be sent and summed in bfloat16 or wider, within the bound.
A program may use at most 64 MiB of HBM per device.

```python
import math
import jax
import jax.numpy as jnp
from jax import lax

D = 2048
H = 16
DK = 128
DV = 128
BLOCK = 64
SEQS = 8
SEG = 128
LEN = 1024


def draw_decay_rate(key, part):
    pick_key, fast_key, slow_key = jax.random.split(jax.random.fold_in(key, 11), 3)
    share = 0.5
    coin = jax.random.uniform(pick_key, (H,), jnp.float32)
    fast = jnp.exp(jax.random.uniform(fast_key, (H,), jnp.float32, math.log(0.04), math.log(0.1)))
    slow = jnp.exp(jax.random.uniform(slow_key, (H,), jnp.float32, math.log(0.05), math.log(0.3))) / LEN
    return jnp.where(coin < share, fast, slow).astype(jnp.float32)


def draw_log_decay_extra(key, part):
    block_key, place_key, depth_key = jax.random.split(jax.random.fold_in(key, 23), 3)
    factor = jnp.exp(jax.random.uniform(block_key, (SEQS, LEN // SEG), jnp.float32, math.log(0.1), math.log(1.0)))
    starting_shift = -jnp.repeat(factor, SEG, axis=1) / LEN
    stored_slots = jax.random.randint(place_key, (SEQS, 2), 0, LEN)
    stack_levels = jax.random.uniform(depth_key, (SEQS, 2), jnp.float32, math.log(0.5), math.log(0.8))
    sequence_indices = jnp.arange(LEN)
    emitted_span = jnp.sum(jnp.where(sequence_indices[None, None, :] == stored_slots[:, :, None], stack_levels[:, :, None], 0.0), axis=1)
    overall_count = starting_shift + emitted_span
    return jnp.broadcast_to(overall_count[:, None, :], (SEQS, H, LEN)).astype(jnp.float32)


def level_of(stream_key, dims, cuts, low, top_value):
    level = 1.0
    for axis_at, blocks in cuts:
        steps = jax.random.uniform(jax.random.fold_in(jax.random.fold_in(stream_key, 6), axis_at), (blocks,), jnp.float32, low / len(cuts), top_value / len(cuts))
        level = level * jnp.repeat(jnp.exp(steps), dims[axis_at] // blocks).reshape((-1,) + (1,) * (len(dims) - 1 - axis_at))
    return level


def noise(key, shape, scale, reach, cuts=(), kind=jnp.bfloat16):
    values = jax.random.normal(key, shape, jnp.float32) * scale
    if len(cuts) > 0:
        values = level_of(key, shape, cuts, -0.22, 0.18) * values
    return jnp.clip(values, min=-reach, max=reach).astype(kind)


def setup_inputs(seed: int = 0) -> dict:
    key_of = jax.random.split(jax.random.key(seed), 10)
    return {
        "layer_input": noise(key_of[0], (SEQS, LEN, D), 1.0, 6.0, ((1, 8), (2, 4))),
        "w_key": noise(key_of[1], (D, H * DK), D ** -0.5, 0.125, ((1, 4),)),
        "w_value": noise(key_of[2], (D, H * DV), D ** -0.5, 0.125, ((1, 4),)),
        "w_gates": noise(key_of[3], (2, D, H), D ** -0.5, 0.125),
        "decay_rate": draw_decay_rate(jax.random.fold_in(key_of[9], 71), 0),
        "beta_bias": jnp.clip(-5.5 + 2.5 * jax.random.uniform(key_of[5], (H,), jnp.float32) ** level_of(key_of[5], (H,), ((0, 4),), -0.2, 0.2), -5.5, -3.0),
        "log_decay_extra": draw_log_decay_extra(jax.random.fold_in(key_of[9], 71), 0),
        "new_query": noise(key_of[7], (SEQS, H * DK), 1.0, 6.0, ((1, 4),)),
        "read_gain": jnp.clip(1.0 + 0.18 * jax.random.normal(key_of[8], (DV,), jnp.float32), 0.1, 1.9),
    }


EPS = 1e-06
HIGH = lax.Precision.HIGHEST

def unit_rows(values):
    return values * lax.rsqrt(lax.optimization_barrier(jnp.sum(values * values, axis=-1, keepdims=True)) + EPS)

def block_pieces(keys, values, log_decay, beta):
    size = keys.shape[-2]
    width = values.shape[-1]
    running = jnp.cumsum(log_decay, axis=-1)
    sequence_indices = jnp.arange(size)
    causal = sequence_indices[:, None] >= sequence_indices[None, :]
    strict = sequence_indices[:, None] > sequence_indices[None, :]
    spread = running[..., :, None] - running[..., None, :]
    weights = jnp.where(causal, jnp.exp(jnp.where(causal, spread, 0.0)), 0.0)
    key_beta = keys * beta[..., None]
    lower = jnp.where(strict, jnp.einsum('...cd,...sd->...cs', key_beta, keys, precision=HIGH) * weights, 0.0)
    right_side = jnp.concatenate([values * beta[..., None], key_beta * jnp.exp(running)[..., None]], axis=-1)
    solved = lax.linalg.triangular_solve(lower, right_side, left_side=True, lower=True, unit_diagonal=True)
    fresh = solved[..., :width]
    erase = solved[..., width:]
    last = running[..., -1]
    key_late = keys * jnp.exp(last[..., None] - running)[..., None]
    identity = jnp.eye(keys.shape[-1], dtype=jnp.float32)
    transition = jnp.exp(last)[..., None, None] * identity - jnp.einsum('...cd,...ce->...de', key_late, erase, precision=HIGH)
    inject = jnp.einsum('...cd,...cv->...dv', key_late, fresh, precision=HIGH)
    return (transition, inject)

def reference(layer_input, w_key, w_value, w_gates, decay_rate, beta_bias, log_decay_extra, new_query, read_gain):
    blocks = LEN // BLOCK

    def one_prompt(pair):
        rows, extra = pair
        key_pre = jnp.dot(rows.astype(jnp.float32), w_key.astype(jnp.float32), preferred_element_type=jnp.float32).reshape(LEN, H, DK)
        value_pre = jnp.dot(rows.astype(jnp.float32), w_value.astype(jnp.float32), preferred_element_type=jnp.float32).reshape(LEN, H, DV)
        decay_pre = jnp.dot(rows.astype(jnp.float32), w_gates[0].astype(jnp.float32), preferred_element_type=jnp.float32)
        beta_pre = jnp.dot(rows.astype(jnp.float32), w_gates[1].astype(jnp.float32), preferred_element_type=jnp.float32)
        keys = unit_rows(jax.nn.silu(key_pre))
        values = jax.nn.silu(value_pre)
        log_decay = -decay_rate[None, :] * jax.nn.softplus(decay_pre) + extra.T
        beta = jax.nn.sigmoid(beta_pre + beta_bias[None, :])
        key_blocks = keys.reshape(blocks, BLOCK, H, DK).transpose(2, 0, 1, 3)
        value_tiles = values.reshape(blocks, BLOCK, H, DV).transpose(2, 0, 1, 3)
        decay_blocks = log_decay.reshape(blocks, BLOCK, H).transpose(2, 0, 1)
        strength_groups = beta.reshape(blocks, BLOCK, H).transpose(2, 0, 1)
        transition, inject = block_pieces(key_blocks, value_tiles, decay_blocks, strength_groups)

        def advance(state, piece):
            block_map, block_add = piece
            return (jnp.einsum('hde,hev->hdv', block_map, state, precision=HIGH) + block_add, None)
        start = jnp.zeros((H, DK, DV), jnp.float32)
        state, _ = lax.scan(advance, start, (jnp.moveaxis(transition, 1, 0), jnp.moveaxis(inject, 1, 0)))
        return state
    final_state = lax.map(one_prompt, (layer_input, log_decay_extra))
    cached = final_state.astype(jnp.bfloat16)
    state_cache = cached.transpose(0, 2, 1, 3).reshape(SEQS * DK, H * DV)
    query = new_query.reshape(SEQS, H, DK).astype(jnp.float32)
    raw_read = jnp.einsum('shav,sha->shv', cached.astype(jnp.float32), query, precision=HIGH)
    scaled = raw_read * lax.rsqrt(lax.optimization_barrier(jnp.mean(raw_read * raw_read, axis=-1, keepdims=True)) + EPS) * read_gain
    first_read = scaled.astype(jnp.bfloat16).reshape(SEQS, H * DV)
    return (state_cache, first_read)
```

```python
import functools

import jax
import jax.numpy as jnp
from jax import lax
from jax.experimental import pallas as pl
from jax.experimental.pallas import tpu as pltpu
from jax.sharding import PartitionSpec as P

DK = 128
DV = 128
EPS = 1e-06
HIGH = lax.Precision.HIGHEST
BF = jnp.bfloat16
F32 = jnp.float32


def dot(left, right, dims=((1,), (0,)), precision=None):
    return lax.dot_general(
        left, right, (dims, ((), ())), precision=precision, preferred_element_type=F32
    )


def kernel(
    n_sp,
    n_tp,
    nh,
    rows,
    x_hbm,
    wk_hbm,
    wv_hbm,
    gates_ref,
    rate_ref,
    bias_ref,
    extra_ref,
    query_ref,
    gain_ref,
    state_out,
    read_out,
    gath,
    w,
    graw,
    level,
    upper,
    maps,
    adds,
    decs,
    pair_maps,
    pair_adds,
    pair_decs,
    joint_decs,
    came,
    sent,
    final,
    landing,
    read_buf,
    read_land,
    query_heads,
    local_sem,
    gsend,
    grecv,
    psend,
    precv,
    csend,
    crecv,
    ssend,
    srecv,
    rsend,
    rrecv,
):
    prompts, seg, depth = x_hbm.shape
    width = nh * DK
    heads = gates_ref.shape[0] // 2
    sp = lax.axis_index("sp")
    tp = lax.axis_index("tp")
    core = lax.rem(sp, 2)
    other = 1 - core
    chip = sp // 2
    last_chip = n_sp // 2 - 1
    share = max(nh // 2, 1)
    mine = core * share
    theirs = other * share
    has_mine = mine < nh
    has_theirs = theirs < nh
    sources = [k for k in range(2) if k * share < nh]
    chunks = DK // rows
    relay = n_tp == 4

    x_copy = pltpu.make_async_copy(x_hbm, gath.at[tp], local_sem.at[0])
    x_copy.start()
    wk_copy = pltpu.make_async_copy(wk_hbm, w.at[:, pl.ds(0, width)], local_sem.at[1])
    wv_copy = pltpu.make_async_copy(wv_hbm, w.at[:, pl.ds(width, nh * DV)], local_sem.at[2])
    wk_copy.start()
    wv_copy.start()

    barrier = pltpu.get_barrier_semaphore()

    def greet_tp(step, carry):
        pl.semaphore_signal(barrier, inc=1, device_id={"tp": lax.rem(tp + step, n_tp)})
        return carry

    def greet_sp(step, carry):
        pl.semaphore_signal(barrier, inc=1, device_id={"sp": lax.rem(sp + step, n_sp)})
        return carry

    lax.fori_loop(1, n_tp, greet_tp, 0)
    lax.fori_loop(1, n_sp, greet_sp, 0)
    r_id = lax.broadcasted_iota(jnp.int32, (seg, seg), 0)
    c_id = lax.broadcasted_iota(jnp.int32, (seg, seg), 1)
    lev = jnp.zeros((seg, seg), jnp.int32)
    k = 1
    while (1 << k) < seg:
        lev = jnp.where((r_id >> k) != (c_id >> k), k, lev)
        k += 1
    levels = k
    level[...] = jnp.where(r_id > c_id, lev, -1)
    upper[...] = jnp.where(r_id <= c_id, 1.0, 0.0).astype(F32)
    graw[...] = jnp.zeros_like(graw)
    pl.semaphore_wait(barrier, n_tp - 1 + n_sp - 1)
    x_copy.wait()

    xn = tp + 1 - 2 * lax.rem(tp, 2)
    yn = tp + 2 - 4 * (tp // 2)
    half = seg // 2

    def direct(p, way):
        target = xn if way == 0 else yn
        return pltpu.make_async_remote_copy(
            src_ref=gath.at[tp, p],
            dst_ref=gath.at[tp, p],
            send_sem=gsend.at[way, p],
            recv_sem=grecv.at[way, p],
            device_id={"tp": target},
        )

    def passed(p, way):
        source = xn if way == 0 else yn
        target = yn if way == 0 else xn
        part = pl.ds(way * half, half)
        return pltpu.make_async_remote_copy(
            src_ref=gath.at[source, p, part],
            dst_ref=gath.at[source, p, part],
            send_sem=gsend.at[2 + way, p],
            recv_sem=grecv.at[2 + way, p],
            device_id={"tp": target},
        )

    def plain(p, step):
        return pltpu.make_async_remote_copy(
            src_ref=gath.at[tp, p],
            dst_ref=gath.at[tp, p],
            send_sem=gsend.at[step, p],
            recv_sem=grecv.at[step, p],
            device_id={"tp": lax.rem(tp + step, n_tp)},
        )

    def start_direct(p):
        direct(p, 0).start()
        direct(p, 1).start()

    def pass_on(p):
        direct(p, 0).wait_recv()
        passed(p, 0).start()
        direct(p, 1).wait_recv()
        passed(p, 1).start()

    early = min(2, prompts)
    ahead = min(1, prompts)
    if relay:
        for p in range(early):
            start_direct(p)
        for p in range(ahead):
            pass_on(p)
            if early + p < prompts:
                start_direct(early + p)
    else:

        def start_plain(index, carry):
            plain(index // (n_tp - 1), lax.rem(index, n_tp - 1) + 1).start()
            return carry

        lax.fori_loop(0, prompts * (n_tp - 1), start_plain, 0)
    wk_copy.wait()
    wv_copy.wait()

    def pair_copies(p):
        pairs = (
            (maps.at[p, pl.ds(theirs, share)], pair_maps.at[p]),
            (adds.at[p, pl.ds(theirs, share)], pair_adds.at[p]),
            (decs.at[p], pair_decs.at[p]),
        )
        return [
            pltpu.make_async_remote_copy(
                src_ref=source,
                dst_ref=target,
                send_sem=psend.at[i, p],
                recv_sem=precv.at[i, p],
                device_id={"sp": sp + 1 - 2 * core},
            )
            for i, (source, target) in enumerate(pairs)
        ]

    def chain_copy(p, j):
        return pltpu.make_async_remote_copy(
            src_ref=sent.at[p, j],
            dst_ref=came.at[p, j],
            send_sem=csend.at[p, j],
            recv_sem=crecv.at[p, j],
            device_id={"sp": lax.rem(sp + 2, n_sp)},
        )

    def state_copy(p, c, slot):
        return pltpu.make_async_remote_copy(
            src_ref=final.at[p, :, pl.ds(c * rows, rows)],
            dst_ref=landing.at[pl.ds(slot * share, share)],
            send_sem=ssend.at[p, c],
            recv_sem=srecv.at[slot],
            device_id={"sp": p * chunks + c},
        )

    def read_copy(target, slot):
        return pltpu.make_async_remote_copy(
            src_ref=read_buf,
            dst_ref=read_land.at[pl.ds(slot * share, share)],
            send_sem=rsend.at[target],
            recv_sem=rrecv.at[slot],
            device_id={"sp": target},
        )

    first_head = tp * nh
    pad = 8
    row_id = lax.broadcasted_iota(jnp.int32, (pad, seg), 0)

    def work(p):
        x = jnp.concatenate([gath[s, p] for s in range(n_tp)], axis=1)
        pre = dot(x, w[...])
        gt = dot(gates_ref[...], x, ((1,), (1,)))
        graw[0, pl.ds(0, heads)] = gt[:heads]
        graw[1, pl.ds(0, heads)] = gt[heads:]
        gd = graw[0, pl.ds(first_head, pad)]
        gb = graw[1, pl.ds(first_head, pad)]
        rate = jnp.zeros((pad, seg), F32)
        bias = jnp.zeros((pad, seg), F32)
        for h in range(nh):
            rate = jnp.where(row_id == h, rate_ref[h], rate)
            bias = jnp.where(row_id == h, bias_ref[h], bias)
        extra = jnp.concatenate([extra_ref[p], jnp.zeros((pad - nh, seg), F32)], axis=0)
        soft = jnp.maximum(gd, 0.0) + jnp.log1p(jnp.exp(-jnp.abs(gd)))
        log_decay = extra - rate * soft
        beta = jax.nn.sigmoid(gb + bias)
        run = dot(log_decay, upper[...], precision=HIGH)
        end = run[:, seg - 1 : seg]
        decs[p] = jnp.broadcast_to(jnp.exp(end), (pad, DV))
        cols = jnp.concatenate(
            [run, beta, beta * jnp.exp(run), jnp.exp(end - run)], axis=0
        ).T
        act = pre * jax.nn.sigmoid(pre)
        lev = level[...]
        strict = lev >= 0
        eye = jnp.where(
            lax.broadcasted_iota(jnp.int32, (seg, seg), 0)
            == lax.broadcasted_iota(jnp.int32, (seg, seg), 1),
            1.0,
            0.0,
        ).astype(F32)
        keys, lower, inv = [], [], []
        for h in range(nh):
            raw = act[:, h * DK : (h + 1) * DK]
            key = raw * lax.rsqrt(jnp.sum(raw * raw, axis=-1, keepdims=True) + EPS)
            kb = key.astype(BF)
            gram = dot(kb, kb, ((1,), (1,)))
            spread = cols[:, h : h + 1] - run[h : h + 1, :]
            weight = jnp.exp(jnp.where(strict, spread, 0.0))
            low = jnp.where(strict, gram * weight * cols[:, pad + h : pad + h + 1], 0.0)
            keys.append(key)
            lower.append(low)
            inv.append(jnp.where(lev == 0, -low, 0.0))
        for step in range(1, levels):
            cuts = [jnp.where(lev == step, low, 0.0) for low in lower]
            full = [(eye + part).astype(BF) for part in inv]
            mids = [dot(cut.astype(BF), f) for cut, f in zip(cuts, full)]
            inv = [
                part - dot(f, mid.astype(BF)) for part, f, mid in zip(inv, full, mids)
            ]
        for h in range(nh):
            value = act[:, width + h * DV : width + (h + 1) * DV]
            side = jnp.concatenate(
                [
                    value * cols[:, pad + h : pad + h + 1],
                    keys[h] * cols[:, 2 * pad + h : 2 * pad + h + 1],
                ],
                axis=1,
            )
            solved = side + dot(inv[h].astype(BF), side.astype(BF))
            late = keys[h] * cols[:, 3 * pad + h : 3 * pad + h + 1]
            late_top = late.astype(BF)
            late_rest = (late - late_top.astype(F32)).astype(BF)
            top = solved.astype(BF)
            rest = (solved[:, :DV] - top[:, :DV].astype(F32)).astype(BF)
            tall = ((0,), (0,))
            both = dot(late_top, top, tall)
            adds[p, h] = (
                both[:, :DV] + dot(late_top, rest, tall) + dot(late_rest, top[:, :DV], tall)
            )
            maps[p, h] = both[:, DV:].astype(BF)

    def unite(p):
        def merge(j, early, late, early_dec, late_dec):
            h = mine + j
            map_0, add_0 = early[0][...], early[1][...]
            map_1, add_1 = late[0][...], late[1][...]
            dec_0 = early_dec[p, pl.ds(h, 1)]
            dec_1 = late_dec[p, pl.ds(h, 1)]
            turn = dot(map_1, jnp.concatenate([map_0, add_0.astype(BF)], axis=1))
            maps[p, h] = (
                dec_1 * map_0.astype(F32) + dec_0 * map_1.astype(F32) - turn[:, :DK]
            ).astype(BF)
            adds[p, h] = dec_1 * add_0 + add_1 - turn[:, DK:]

        @pl.when(has_mine)
        def _():
            for copy in pair_copies(p):
                copy.wait_recv()
            joint_decs[p] = decs[p] * pair_decs[p]
            for first in range(2):

                @pl.when(core == first)
                def _():
                    for j in range(share):
                        own = (maps.at[p, mine + j], adds.at[p, mine + j])
                        got = (pair_maps.at[p, j], pair_adds.at[p, j])
                        if first == 0:
                            merge(j, own, got, decs, pair_decs)
                        else:
                            merge(j, got, own, pair_decs, decs)

    def advance(p):
        @pl.when(chip == 0)
        def _():
            for j in range(share):
                sent[p, j] = adds[p, mine + j].astype(BF)
                chain_copy(p, j).start()

        def moved(j):
            chain_copy(p, j).wait_recv()
            state = came[p, j]
            h = mine + j
            return (
                joint_decs[p, pl.ds(h, 1)] * state.astype(F32)
                + adds[p, h]
                - dot(maps[p, h], state)
            )

        @pl.when(jnp.logical_and(chip > 0, chip < last_chip))
        def _():
            for j in range(share):
                sent[p, j] = moved(j).astype(BF)
                chain_copy(p, j).start()

        @pl.when(chip == last_chip)
        def _():
            for j in range(share):
                state = moved(j).astype(BF)
                final[p, j] = state
                raw = dot(query_heads[mine + j], state)
                norm = (
                    raw
                    * lax.rsqrt(jnp.mean(raw * raw, axis=-1, keepdims=True) + EPS)
                    * gain_ref[...]
                )
                at_p = lax.broadcasted_iota(jnp.int32, norm.shape, 0) == p
                read_buf[j] = jnp.where(at_p, norm, read_buf[j])
            for c in range(chunks):
                owner = p * chunks + c

                @pl.when(owner != sp)
                def _():
                    state_copy(p, c, core).start()

                @pl.when(owner == sp)
                def _():
                    for j in range(share):
                        landing[mine + j] = final[p, j, c * rows : (c + 1) * rows]

    ending = jnp.logical_and(chip == last_chip, has_mine)

    @pl.when(ending)
    def _():
        read_buf[...] = jnp.zeros_like(read_buf)
        for h in range(nh):
            query_heads[h] = query_ref[:, h * DK : (h + 1) * DK]

    lag = 1 + chip

    def body(it, carry):
        if relay:

            @pl.when(it + ahead < prompts)
            def _():
                pass_on(it + ahead)

            @pl.when(it + ahead + early < prompts)
            def _():
                start_direct(it + ahead + early)

        @pl.when(it < prompts)
        def _():
            if relay:
                passed(it, 0).wait_recv()
                passed(it, 1).wait_recv()
            else:

                def take(step, carry):
                    plain(it, step).wait_recv()
                    return carry

                lax.fori_loop(1, n_tp, take, 0)
            work(it)

            @pl.when(has_theirs)
            def _():
                for copy in pair_copies(it):
                    copy.start()

        @pl.when(jnp.logical_and(it >= 1, it < prompts + 1))
        def _():
            unite(it - 1)

        moving = jnp.logical_and(it >= lag, it < prompts + lag)

        @pl.when(jnp.logical_and(moving, has_mine))
        def _():
            advance(it - lag)

        return carry

    lax.fori_loop(0, prompts + last_chip + 1, body, 0)

    @pl.when(ending)
    def _():
        def tell(target, carry):
            @pl.when(target != sp)
            def _():
                read_copy(target, core).start()

            return carry

        lax.fori_loop(0, n_sp, tell, 0)
        for j in range(share):
            read_land[mine + j] = read_buf[j]

    for k in sources:

        @pl.when(sp != 2 * last_chip + k)
        def _():
            state_copy(0, 0, k).wait_recv()
            read_copy(0, k).wait_recv()

    for h in range(nh):
        state_out[:, h * DV : (h + 1) * DV] = landing[h]
        read_out[:, h * DV : (h + 1) * DV] = read_land[h].astype(BF)

    @pl.when(ending)
    def _():
        def told(target, carry):
            @pl.when(target != sp)
            def _():
                read_copy(target, core).wait_send()
                state_copy(target // chunks, lax.rem(target, chunks), core).wait_send()

            return carry

        lax.fori_loop(0, n_sp, told, 0)

    @pl.when(jnp.logical_and(chip < last_chip, has_mine))
    def _():
        def left(index, carry):
            chain_copy(index // share, lax.rem(index, share)).wait_send()
            return carry

        lax.fori_loop(0, prompts * share, left, 0)

    @pl.when(has_theirs)
    def _():
        def lent(index, carry):
            for copy in pair_copies(index):
                copy.wait_send()
            return carry

        lax.fori_loop(0, prompts, lent, 0)

    def freed(index, carry):
        if relay:
            direct(index, 0).wait_send()
            direct(index, 1).wait_send()
            passed(index, 0).wait_send()
            passed(index, 1).wait_send()
        else:
            for step in range(1, n_tp):
                plain(index, step).wait_send()
        return carry

    lax.fori_loop(0, prompts, freed, 0)


def near(
    n_sp,
    n_tp,
    nh,
    x_hbm,
    wk_hbm,
    wv_hbm,
    gates_ref,
    rate_ref,
    bias_ref,
    extra_ref,
    query_ref,
    gain_ref,
    state_out,
    read_out,
    gath,
    w,
    gall,
    gsel,
    fixed,
    level,
    upper,
    acc,
    gacc,
    maps,
    adds,
    decs,
    up_out,
    up_in,
    map_out,
    map_in,
    add_out,
    add_in,
    dec_out,
    dec_in,
    query,
    read_buf,
    read_land,
    local_sem,
    gsend,
    grecv,
    usend,
    urecv,
    dsend,
    drecv,
    rsend,
    rrecv,
):
    prompts, seg, depth = x_hbm.shape
    width = nh * DK
    heads = gates_ref.shape[0] // 2
    pad = 8
    last = n_sp - 1
    sp = lax.axis_index("sp")
    tp = lax.axis_index("tp")
    core = lax.rem(sp, 2)

    x_copy = pltpu.make_async_copy(x_hbm, gath.at[tp], local_sem.at[0])
    x_copy.start()
    wk_copy = pltpu.make_async_copy(wk_hbm, w.at[:, pl.ds(0, width)], local_sem.at[1])
    wv_copy = pltpu.make_async_copy(wv_hbm, w.at[:, pl.ds(width, nh * DV)], local_sem.at[2])
    wk_copy.start()
    wv_copy.start()

    barrier = pltpu.get_barrier_semaphore()
    xn = tp + 1 - 2 * lax.rem(tp, 2)
    yn = tp + 2 - 4 * (tp // 2)
    far = n_tp - 1 - tp

    pl.semaphore_signal(barrier, inc=1, device_id={"tp": xn})
    pl.semaphore_signal(barrier, inc=1, device_id={"tp": yn})

    def greet_sp(step, carry):
        pl.semaphore_signal(barrier, inc=1, device_id={"sp": lax.rem(sp + step, n_sp)})
        return carry

    lax.fori_loop(1, n_sp, greet_sp, 0)

    r_id = lax.broadcasted_iota(jnp.int32, (seg, seg), 0)
    c_id = lax.broadcasted_iota(jnp.int32, (seg, seg), 1)
    lev = jnp.zeros((seg, seg), jnp.int32)
    k = 1
    while (1 << k) < seg:
        lev = jnp.where((r_id >> k) != (c_id >> k), k, lev)
        k += 1
    levels = k
    level[...] = jnp.where(r_id > c_id, lev, -1)
    upper[...] = jnp.where(r_id <= c_id, 1.0, 0.0).astype(BF)
    groups = [(k, min(k + 3, levels)) for k in range(1, levels, 3)]

    row_id = lax.broadcasted_iota(jnp.int32, (pad, seg), 0)
    rate = jnp.zeros((pad, seg), F32)
    bias = jnp.zeros((pad, seg), F32)
    for h in range(nh):
        rate = jnp.where(row_id == h, rate_ref[h], rate)
        bias = jnp.where(row_id == h, bias_ref[h], bias)
    fixed[0] = rate
    fixed[1] = bias
    for at in range(n_tp * depth // 128):
        part = gates_ref[:, at * 128 : (at + 1) * 128].astype(F32)
        gall[at, pl.ds(0, heads)] = part[:heads]
        gall[at, pl.ds(heads, heads)] = part[heads:]
        gall[at, pl.ds(2 * heads, pad)] = jnp.zeros((pad, 128), F32)
        picked = [gall[at, pl.ds(tp * nh + k * heads, pad)] for k in range(2)]
        gsel[:, at * 128 : (at + 1) * 128] = jnp.concatenate(picked, axis=0).astype(BF)
    every = query_ref[...].astype(F32)
    mine = lax.broadcasted_iota(jnp.int32, every.shape, 0) == sp
    asked = jnp.sum(jnp.where(mine, every, 0.0), axis=0, keepdims=True)
    for h in range(nh):
        query[h] = jnp.broadcast_to(asked[:, h * DK : (h + 1) * DK], (pad, DK))
    read_buf[...] = jnp.zeros_like(read_buf)

    @pl.when(core == 0)
    def _():
        up_in[:, 1] = jnp.zeros((n_sp - 1, nh, DK, DV), BF)

    @pl.when(core == 1)
    def _():
        add_in[:, 1] = jnp.zeros((n_sp - 1, nh, DK, DV), BF)

    pl.semaphore_wait(barrier, 2 + n_sp - 1)
    x_copy.wait()

    half = seg // 2

    def prompt_at(t):
        rev = last - t
        p = 0
        k = 1
        while k < n_sp:
            p = p + k * lax.rem(sp // k + rev // k, 2)
            k *= 2
        return p

    def direct(t, way):
        p = prompt_at(t)
        return pltpu.make_async_remote_copy(
            src_ref=gath.at[tp, p],
            dst_ref=gath.at[tp, p],
            send_sem=gsend.at[way, t],
            recv_sem=grecv.at[way, t],
            device_id={"tp": xn if way == 0 else yn},
        )

    def passed(t, way):
        p = prompt_at(t)
        source = xn if way == 0 else yn
        part = pl.ds(way * half, half)
        return pltpu.make_async_remote_copy(
            src_ref=gath.at[source, p, part],
            dst_ref=gath.at[source, p, part],
            send_sem=gsend.at[2 + way, t],
            recv_sem=grecv.at[2 + way, t],
            device_id={"tp": yn if way == 0 else xn},
        )

    def start_direct(t):
        direct(t, 0).start()
        direct(t, 1).start()

    def pass_on(t):
        direct(t, 0).wait_recv()
        passed(t, 0).start()
        direct(t, 1).wait_recv()
        passed(t, 1).start()

    def up_copy(t, part):
        return pltpu.make_async_remote_copy(
            src_ref=up_out.at[t, part],
            dst_ref=up_in.at[t, part],
            send_sem=usend.at[part, t],
            recv_sem=urecv.at[part, t],
            device_id={"sp": sp + 1},
        )

    def down_copy(t, part):
        pairs = (
            (map_out.at[t], map_in.at[t]),
            (add_out.at[t, 0], add_in.at[t, 0]),
            (dec_out.at[t], dec_in.at[t]),
            (add_out.at[t, 1], add_in.at[t, 1]),
        )
        return pltpu.make_async_remote_copy(
            src_ref=pairs[part][0],
            dst_ref=pairs[part][1],
            send_sem=dsend.at[part, t],
            recv_sem=drecv.at[part, t],
            device_id={"sp": sp - 1},
        )

    def read_copy(target, source):
        return pltpu.make_async_remote_copy(
            src_ref=read_buf,
            dst_ref=read_land.at[source],
            send_sem=rsend.at[target],
            recv_sem=rrecv.at[source],
            device_id={"sp": target},
        )

    def band(source):
        return pl.ds(pl.multiple_of(source * depth, depth), depth)

    tile = DK + DV
    near_by = (tp, xn, yn)

    def ahead(t):
        p = prompt_at(t)
        slot = lax.rem(t, 2)
        x = jnp.concatenate([gath[s, p] for s in near_by], axis=1)

        def gate_piece():
            g = jnp.concatenate([gsel[:, band(s)] for s in near_by], axis=1)
            gacc[slot] = dot(g, x, ((1,), (1,)))

        def piece(at):
            def go():
                cols = pl.ds(at * tile, tile)
                side = jnp.concatenate([w[band(s), cols] for s in near_by], axis=0)
                acc[slot, :, cols] = dot(x, side)

            return go

        return [gate_piece] + [piece(at) for at in range(2 * width // tile)]

    def work(t, pieces):
        pieces = list(pieces)

        def fill():
            if pieces:
                pieces.pop(0)()

        p = prompt_at(t)
        slot = lax.rem(t, 2)
        x = gath[far, p]
        gt = gacc[slot] + dot(gsel[:, band(far)], x, ((1,), (1,)))
        key_pre = acc[slot, :, :width] + dot(x, w[band(far), :width])
        value_pre = acc[slot, :, width:] + dot(x, w[band(far), width:])
        gd = gt[:pad]
        gb = gt[pad:]
        extra = jnp.concatenate([extra_ref[p], jnp.zeros((pad - nh, seg), F32)], axis=0)
        soft = jnp.maximum(gd, 0.0) + jnp.log1p(jnp.exp(-jnp.abs(gd)))
        log_decay = extra - fixed[0] * soft
        beta = jax.nn.sigmoid(gb + fixed[1])
        high = log_decay.astype(BF).astype(F32)
        rest = log_decay - high
        mid = rest.astype(BF).astype(F32)
        split = jnp.concatenate([high, mid, rest - mid, jnp.zeros_like(high)], axis=0)
        sums = dot(split.astype(BF), upper[...])
        run = sums[:pad] + sums[pad : 2 * pad] + sums[2 * pad : 3 * pad]
        end = run[:, seg - 1 : seg]
        decs[p] = jnp.broadcast_to(jnp.exp(end), (pad, DV))
        cols = jnp.concatenate(
            [run, beta, beta * jnp.exp(run), jnp.exp(end - run)], axis=0
        ).T
        lev = level[...]
        strict = lev >= 0
        eye = jnp.where(
            lax.broadcasted_iota(jnp.int32, (seg, seg), 0)
            == lax.broadcasted_iota(jnp.int32, (seg, seg), 1),
            1.0,
            0.0,
        ).astype(F32)
        hs = range(nh)
        keys, grams = [], []
        for h in hs:
            pre = key_pre[:, h * DK : (h + 1) * DK]
            raw = pre * jax.nn.sigmoid(pre)
            key = raw * lax.rsqrt(jnp.sum(raw * raw, axis=-1, keepdims=True) + EPS)
            kb = key.astype(BF)
            keys.append(key)
            grams.append(dot(kb, kb, ((1,), (1,))))
        fill()
        fill()
        lower, inv = [], []
        for h in hs:
            spread = cols[:, h : h + 1] - run[h : h + 1, :]
            weight = jnp.exp(jnp.where(strict, spread, 0.0))
            low = jnp.where(strict, grams[h] * weight * cols[:, pad + h : pad + h + 1], 0.0)
            lower.append(low)
            inv.append(eye - jnp.where(lev == 0, low, 0.0))

        def merge(first, until):
            inside = jnp.logical_and(lev >= first, lev < until)
            cuts = [jnp.where(inside, low, 0.0).astype(BF) for low in lower]
            return [dot(f.astype(BF), cut).astype(BF) for f, cut in zip(inv, cuts)]

        for first, until in groups[:-1]:
            steps = merge(first, until)
            fill()
            inv = [f - dot(e, f.astype(BF)) for e, f in zip(steps, inv)]
            for _ in range(first + 1, until):
                steps = [dot(e, e).astype(BF) for e in steps]
                fill()
                inv = [f + dot(e, f.astype(BF)) for e, f in zip(steps, inv)]
        sides = []
        for h in hs:
            pre = value_pre[:, h * DV : (h + 1) * DV]
            value = pre * jax.nn.sigmoid(pre)
            sides.append(
                jnp.concatenate(
                    [
                        value * cols[:, pad + h : pad + h + 1],
                        keys[h] * cols[:, 2 * pad + h : 2 * pad + h + 1],
                    ],
                    axis=1,
                )
            )
        first, until = groups[-1]
        steps = merge(first, until)
        sides = [
            side + dot((f - eye).astype(BF), side.astype(BF)) for f, side in zip(inv, sides)
        ]
        fill()
        sides = [side - dot(e, side.astype(BF)) for e, side in zip(steps, sides)]
        for _ in range(first + 1, until):
            steps = [dot(e, e).astype(BF) for e in steps]
            fill()
            sides = [side + dot(e, side.astype(BF)) for e, side in zip(steps, sides)]
        while pieces:
            fill()
        tall = ((0,), (0,))
        for h in hs:
            late = keys[h] * cols[:, 3 * pad + h : 3 * pad + h + 1]
            late_top = late.astype(BF)
            late_rest = (late - late_top.astype(F32)).astype(BF)
            top = sides[h].astype(BF)
            rest = (sides[h][:, :DV] - top[:, :DV].astype(F32)).astype(BF)
            both = dot(late_top, top, tall)
            adds[p, h] = (
                both[:, :DV] + dot(late_top, rest, tall) + dot(late_rest, top[:, :DV], tall)
            )
            maps[p, h] = both[:, DV:].astype(BF)

    def moved(at, p, h):
        top = up_in[at, 0, h]
        state = top.astype(F32) + up_in[at, 1, h].astype(F32)
        return decs[p, pl.ds(h, 1)] * state + adds[p, h] - dot(maps[p, h], top)

    def go_up(t, p, fresh):
        for h in range(nh):
            state = adds[p, h] if fresh else moved(t - 1, p, h)
            top = state.astype(BF)
            up_out[t, 0, h] = top
            up_out[t, 1, h] = (state - top.astype(F32)).astype(BF)

    def go_down(t, p, fresh):
        for h in range(nh):
            if fresh:
                total = adds[p, h]
                map_out[t, h] = maps[p, h]
            else:
                own = decs[p, pl.ds(h, 1)]
                later = dec_in[t - 1, pl.ds(h, 1)]
                late = map_in[t - 1, h]
                early = maps[p, h]
                add = adds[p, h]
                turn = dot(late, jnp.concatenate([early, add.astype(BF)], axis=1))
                total = (
                    later * add
                    + add_in[t - 1, 0, h].astype(F32)
                    + add_in[t - 1, 1, h].astype(F32)
                    - turn[:, DK:]
                )
                map_out[t, h] = (
                    later * early.astype(F32) + own * late.astype(F32) - turn[:, :DK]
                ).astype(BF)
            top = total.astype(BF)
            add_out[t, 0, h] = top
            add_out[t, 1, h] = (total - top.astype(F32)).astype(BF)
        dec_out[t] = decs[p] if fresh else decs[p] * dec_in[t - 1]

    def wait_up(t):
        up_copy(t, 0).wait_recv()

        @pl.when(core == 1)
        def _():
            up_copy(t, 1).wait_recv()

    def wait_down(t):
        for part in range(3):
            down_copy(t, part).wait_recv()

        @pl.when(core == 0)
        def _():
            down_copy(t, 3).wait_recv()

    def chain(t):
        rev = last - t

        @pl.when(sp + rev <= last)
        def _():
            @pl.when(sp == 0)
            def _():
                go_up(t, rev, True)

            @pl.when(sp > 0)
            def _():
                wait_up(t - 1)
                go_up(t, sp + rev, False)

            up_copy(t, 0).start()

            @pl.when(core == 0)
            def _():
                up_copy(t, 1).start()

        @pl.when(sp >= rev)
        def _():
            @pl.when(sp == last)
            def _():
                go_down(t, last - rev, True)

            @pl.when(sp < last)
            def _():
                wait_down(t - 1)
                go_down(t, sp - rev, False)

            for part in range(3):
                down_copy(t, part).start()

            @pl.when(core == 1)
            def _():
                down_copy(t, 3).start()

    def close(below, above):
        at = last - 1
        for h in range(nh):
            state = moved(at, sp, h) if below else adds[sp, h]
            if above:
                state = (
                    dec_in[at, pl.ds(h, 1)] * state
                    + add_in[at, 0, h].astype(F32)
                    + add_in[at, 1, h].astype(F32)
                    - dot(map_in[at, h], state.astype(BF))
                )
            cached = state.astype(BF)
            state_out[:, h * DV : (h + 1) * DV] = cached
            raw = dot(query[h].astype(BF), cached)
            norm = (
                raw
                * lax.rsqrt(jnp.mean(raw * raw, axis=-1, keepdims=True) + EPS)
                * gain_ref[...]
            )
            read_buf[pl.ds(h, 1)] = norm[:1]

    early = min(2, prompts)
    for t in range(early):
        start_direct(t)
    pass_on(0)
    if early < prompts:
        start_direct(early)
    wk_copy.wait()
    wv_copy.wait()
    for go in ahead(0):
        go()

    def body(t, carry):
        pass_on(t + 1)

        @pl.when(t + 1 + early < prompts)
        def _():
            start_direct(t + 1 + early)

        passed(t, 0).wait_recv()
        passed(t, 1).wait_recv()
        work(t, ahead(t + 1))
        chain(t)
        return carry

    lax.fori_loop(0, last, body, 0)
    passed(last, 0).wait_recv()
    passed(last, 1).wait_recv()
    work(last, [])

    @pl.when(sp > 0)
    def _():
        wait_up(last - 1)

    @pl.when(sp < last)
    def _():
        wait_down(last - 1)

    @pl.when(sp == 0)
    def _():
        close(False, True)

    @pl.when(jnp.logical_and(sp > 0, sp < last))
    def _():
        close(True, True)

    @pl.when(sp == last)
    def _():
        close(True, False)

    def tell(step, carry):
        target = lax.rem(sp + step, n_sp)
        read_copy(target, sp).start()
        return carry

    lax.fori_loop(1, n_sp, tell, 0)
    read_land[sp] = read_buf[...]

    def freed(t, carry):
        for way in range(2):
            direct(t, way).wait_send()
            passed(t, way).wait_send()
        return carry

    lax.fori_loop(0, prompts, freed, 0)

    def sent(t, carry):
        rev = last - t

        @pl.when(sp + rev <= last)
        def _():
            up_copy(t, 0).wait_send()

            @pl.when(core == 0)
            def _():
                up_copy(t, 1).wait_send()

        @pl.when(sp >= rev)
        def _():
            for part in range(3):
                down_copy(t, part).wait_send()

            @pl.when(core == 1)
            def _():
                down_copy(t, 3).wait_send()

        return carry

    lax.fori_loop(0, last, sent, 0)

    def told(step, carry):
        source = lax.rem(sp + step, n_sp)
        read_copy(source, source).wait_recv()
        read_copy(source, sp).wait_send()
        return carry

    lax.fori_loop(1, n_sp, told, 0)
    for h in range(nh):
        read_out[:, h * DV : (h + 1) * DV] = read_land[:, h].astype(BF)


def close_by(n_sp, n_tp, prompts, seg, rows, nh):
    even = n_sp >= 2 and n_sp & (n_sp - 1) == 0 and seg & (seg - 1) == 0
    return even and n_tp == 4 and prompts == n_sp and rows == DK and nh <= 8 and seg >= 8


def shards(
    n_sp,
    n_tp,
    layer_input,
    w_key,
    w_value,
    w_gates,
    decay_rate,
    beta_bias,
    log_decay_extra,
    new_query,
    read_gain,
):
    prompts, seg, depth = layer_input.shape
    whole_depth, width = w_key.shape
    nh = width // DK
    heads = w_gates.shape[2]
    rows = prompts * DK // n_sp
    share = max(nh // 2, 1)
    gates = jnp.swapaxes(w_gates, 1, 2).reshape(2 * heads, whole_depth)
    vmem = pl.BlockSpec(memory_space=pltpu.VMEM)
    smem = pl.BlockSpec(memory_space=pltpu.SMEM)
    hbm = pl.BlockSpec(memory_space=pl.ANY)
    dma = pltpu.SemaphoreType.DMA
    if close_by(n_sp, n_tp, prompts, seg, rows, nh):
        hops = n_sp - 1
        return pl.pallas_call(
            functools.partial(near, n_sp, n_tp, nh),
            out_shape=(
                jax.ShapeDtypeStruct((rows, nh * DV), BF),
                jax.ShapeDtypeStruct((prompts, nh * DV), BF),
            ),
            in_specs=[hbm, hbm, hbm, vmem, smem, smem, vmem, vmem, vmem],
            out_specs=(vmem, vmem),
            scratch_shapes=[
                pltpu.VMEM((n_tp, prompts, seg, depth), BF),
                pltpu.VMEM((whole_depth, nh * (DK + DV)), BF),
                pltpu.VMEM((whole_depth // 128, 2 * heads + 8, 128), F32),
                pltpu.VMEM((16, whole_depth), BF),
                pltpu.VMEM((2, 8, seg), F32),
                pltpu.VMEM((seg, seg), jnp.int32),
                pltpu.VMEM((seg, seg), BF),
                pltpu.VMEM((2, seg, nh * (DK + DV)), F32),
                pltpu.VMEM((2, 16, seg), F32),
                pltpu.VMEM((prompts, nh, DK, DK), BF),
                pltpu.VMEM((prompts, nh, DK, DV), F32),
                pltpu.VMEM((prompts, 8, DV), F32),
                pltpu.VMEM((hops, 2, nh, DK, DV), BF),
                pltpu.VMEM((hops, 2, nh, DK, DV), BF),
                pltpu.VMEM((hops, nh, DK, DK), BF),
                pltpu.VMEM((hops, nh, DK, DK), BF),
                pltpu.VMEM((hops, 2, nh, DK, DV), BF),
                pltpu.VMEM((hops, 2, nh, DK, DV), BF),
                pltpu.VMEM((hops, 8, DV), F32),
                pltpu.VMEM((hops, 8, DV), F32),
                pltpu.VMEM((nh, 8, DK), F32),
                pltpu.VMEM((8, DV), F32),
                pltpu.VMEM((prompts, 8, DV), F32),
                dma((3,)),
                dma((4, prompts)),
                dma((4, prompts)),
                dma((2, hops)),
                dma((2, hops)),
                dma((4, hops)),
                dma((4, hops)),
                dma((n_sp,)),
                dma((n_sp,)),
            ],
            compiler_params=pltpu.CompilerParams(
                collective_id=0, has_side_effects=True, vmem_limit_bytes=56 * 1024 * 1024
            ),
        )(
            layer_input,
            w_key,
            w_value,
            gates,
            decay_rate,
            beta_bias,
            log_decay_extra,
            new_query,
            read_gain.reshape(1, DV),
        )
    return pl.pallas_call(
        functools.partial(kernel, n_sp, n_tp, nh, rows),
        out_shape=(
            jax.ShapeDtypeStruct((rows, nh * DV), BF),
            jax.ShapeDtypeStruct((prompts, nh * DV), BF),
        ),
        in_specs=[hbm, hbm, hbm, vmem, smem, smem, vmem, vmem, vmem],
        out_specs=(vmem, vmem),
        scratch_shapes=[
            pltpu.VMEM((n_tp, prompts, seg, depth), BF),
            pltpu.VMEM((whole_depth, nh * (DK + DV)), BF),
            pltpu.VMEM((2, heads + 8, seg), F32),
            pltpu.VMEM((seg, seg), jnp.int32),
            pltpu.VMEM((seg, seg), F32),
            pltpu.VMEM((prompts, nh, DK, DK), BF),
            pltpu.VMEM((prompts, nh, DK, DV), F32),
            pltpu.VMEM((prompts, 8, DV), F32),
            pltpu.VMEM((prompts, share, DK, DK), BF),
            pltpu.VMEM((prompts, share, DK, DV), F32),
            pltpu.VMEM((prompts, 8, DV), F32),
            pltpu.VMEM((prompts, 8, DV), F32),
            pltpu.VMEM((prompts, share, DK, DV), BF),
            pltpu.VMEM((prompts, share, DK, DV), BF),
            pltpu.VMEM((prompts, share, DK, DV), BF),
            pltpu.VMEM((nh, rows, DV), BF),
            pltpu.VMEM((share, prompts, DV), F32),
            pltpu.VMEM((nh, prompts, DV), F32),
            pltpu.VMEM((nh, prompts, DK), BF),
            dma((3,)),
            dma((max(n_tp, 4), prompts)),
            dma((max(n_tp, 4), prompts)),
            dma((3, prompts)),
            dma((3, prompts)),
            dma((prompts, share)),
            dma((prompts, share)),
            dma((prompts, DK // rows)),
            dma((2,)),
            dma((n_sp,)),
            dma((2,)),
        ],
        compiler_params=pltpu.CompilerParams(
            collective_id=0, has_side_effects=True, vmem_limit_bytes=56 * 1024 * 1024
        ),
    )(
        layer_input,
        w_key,
        w_value,
        gates,
        decay_rate,
        beta_bias,
        log_decay_extra,
        new_query,
        read_gain.reshape(1, DV),
    )


def solution(mesh):
    return jax.shard_map(
        functools.partial(shards, mesh.shape["sp"], mesh.shape["tp"]),
        mesh=mesh,
        in_specs=(
            P(None, "sp", "tp"),
            P(None, "tp"),
            P(None, "tp"),
            P(),
            P("tp"),
            P("tp"),
            P(None, "tp", "sp"),
            P(None, "tp"),
            P(),
        ),
        out_specs=(P("sp", "tp"), P(None, "tp")),
        check_vma=False,
    )
```

```python
import functools

import jax
import jax.numpy as jnp
from jax import lax
from jax.experimental import pallas as pl
from jax.experimental.pallas import tpu as pltpu
from jax.sharding import PartitionSpec as P

DK = 128
DV = 128
EPS = 1e-06
HIGH = lax.Precision.HIGHEST
BF = jnp.bfloat16
F32 = jnp.float32


def dot(left, right, dims=((1,), (0,)), precision=None):
    return lax.dot_general(
        left, right, (dims, ((), ())), precision=precision, preferred_element_type=F32
    )


def kernel(
    n_sp,
    n_tp,
    nh,
    rows,
    x_hbm,
    wk_hbm,
    wv_hbm,
    gates_ref,
    rate_ref,
    bias_ref,
    extra_ref,
    query_ref,
    gain_ref,
    state_out,
    read_out,
    gath,
    w,
    graw,
    level,
    upper,
    maps,
    adds,
    decs,
    pair_maps,
    pair_adds,
    pair_decs,
    joint_decs,
    came,
    sent,
    final,
    landing,
    read_buf,
    read_land,
    query_heads,
    local_sem,
    gsend,
    grecv,
    psend,
    precv,
    csend,
    crecv,
    ssend,
    srecv,
    rsend,
    rrecv,
):
    prompts, seg, depth = x_hbm.shape
    width = nh * DK
    heads = gates_ref.shape[0] // 2
    sp = lax.axis_index("sp")
    tp = lax.axis_index("tp")
    core = lax.rem(sp, 2)
    other = 1 - core
    chip = sp // 2
    last_chip = n_sp // 2 - 1
    share = max(nh // 2, 1)
    mine = core * share
    theirs = other * share
    has_mine = mine < nh
    has_theirs = theirs < nh
    sources = [k for k in range(2) if k * share < nh]
    chunks = DK // rows
    relay = n_tp == 4

    x_copy = pltpu.make_async_copy(x_hbm, gath.at[tp], local_sem.at[0])
    x_copy.start()
    wk_copy = pltpu.make_async_copy(wk_hbm, w.at[:, pl.ds(0, width)], local_sem.at[1])
    wv_copy = pltpu.make_async_copy(wv_hbm, w.at[:, pl.ds(width, nh * DV)], local_sem.at[2])
    wk_copy.start()
    wv_copy.start()

    barrier = pltpu.get_barrier_semaphore()

    def greet_tp(step, carry):
        pl.semaphore_signal(barrier, inc=1, device_id={"tp": lax.rem(tp + step, n_tp)})
        return carry

    def greet_sp(step, carry):
        pl.semaphore_signal(barrier, inc=1, device_id={"sp": lax.rem(sp + step, n_sp)})
        return carry

    lax.fori_loop(1, n_tp, greet_tp, 0)
    lax.fori_loop(1, n_sp, greet_sp, 0)
    r_id = lax.broadcasted_iota(jnp.int32, (seg, seg), 0)
    c_id = lax.broadcasted_iota(jnp.int32, (seg, seg), 1)
    lev = jnp.zeros((seg, seg), jnp.int32)
    k = 1
    while (1 << k) < seg:
        lev = jnp.where((r_id >> k) != (c_id >> k), k, lev)
        k += 1
    levels = k
    level[...] = jnp.where(r_id > c_id, lev, -1)
    upper[...] = jnp.where(r_id <= c_id, 1.0, 0.0).astype(F32)
    graw[...] = jnp.zeros_like(graw)
    pl.semaphore_wait(barrier, n_tp - 1 + n_sp - 1)
    x_copy.wait()

    xn = tp + 1 - 2 * lax.rem(tp, 2)
    yn = tp + 2 - 4 * (tp // 2)
    half = seg // 2

    def direct(p, way):
        target = xn if way == 0 else yn
        return pltpu.make_async_remote_copy(
            src_ref=gath.at[tp, p],
            dst_ref=gath.at[tp, p],
            send_sem=gsend.at[way, p],
            recv_sem=grecv.at[way, p],
            device_id={"tp": target},
        )

    def passed(p, way):
        source = xn if way == 0 else yn
        target = yn if way == 0 else xn
        part = pl.ds(way * half, half)
        return pltpu.make_async_remote_copy(
            src_ref=gath.at[source, p, part],
            dst_ref=gath.at[source, p, part],
            send_sem=gsend.at[2 + way, p],
            recv_sem=grecv.at[2 + way, p],
            device_id={"tp": target},
        )

    def plain(p, step):
        return pltpu.make_async_remote_copy(
            src_ref=gath.at[tp, p],
            dst_ref=gath.at[tp, p],
            send_sem=gsend.at[step, p],
            recv_sem=grecv.at[step, p],
            device_id={"tp": lax.rem(tp + step, n_tp)},
        )

    def start_direct(p):
        direct(p, 0).start()
        direct(p, 1).start()

    def pass_on(p):
        direct(p, 0).wait_recv()
        passed(p, 0).start()
        direct(p, 1).wait_recv()
        passed(p, 1).start()

    early = min(2, prompts)
    ahead = min(1, prompts)
    if relay:
        for p in range(early):
            start_direct(p)
        for p in range(ahead):
            pass_on(p)
            if early + p < prompts:
                start_direct(early + p)
    else:

        def start_plain(index, carry):
            plain(index // (n_tp - 1), lax.rem(index, n_tp - 1) + 1).start()
            return carry

        lax.fori_loop(0, prompts * (n_tp - 1), start_plain, 0)
    wk_copy.wait()
    wv_copy.wait()

    def pair_copies(p):
        pairs = (
            (maps.at[p, pl.ds(theirs, share)], pair_maps.at[p]),
            (adds.at[p, pl.ds(theirs, share)], pair_adds.at[p]),
            (decs.at[p], pair_decs.at[p]),
        )
        return [
            pltpu.make_async_remote_copy(
                src_ref=source,
                dst_ref=target,
                send_sem=psend.at[i, p],
                recv_sem=precv.at[i, p],
                device_id={"sp": sp + 1 - 2 * core},
            )
            for i, (source, target) in enumerate(pairs)
        ]

    def chain_copy(p, j):
        return pltpu.make_async_remote_copy(
            src_ref=sent.at[p, j],
            dst_ref=came.at[p, j],
            send_sem=csend.at[p, j],
            recv_sem=crecv.at[p, j],
            device_id={"sp": lax.rem(sp + 2, n_sp)},
        )

    def state_copy(p, c, slot):
        return pltpu.make_async_remote_copy(
            src_ref=final.at[p, :, pl.ds(c * rows, rows)],
            dst_ref=landing.at[pl.ds(slot * share, share)],
            send_sem=ssend.at[p, c],
            recv_sem=srecv.at[slot],
            device_id={"sp": p * chunks + c},
        )

    def read_copy(target, slot):
        return pltpu.make_async_remote_copy(
            src_ref=read_buf,
            dst_ref=read_land.at[pl.ds(slot * share, share)],
            send_sem=rsend.at[target],
            recv_sem=rrecv.at[slot],
            device_id={"sp": target},
        )

    first_head = tp * nh
    pad = 8
    row_id = lax.broadcasted_iota(jnp.int32, (pad, seg), 0)

    def work(p):
        x = jnp.concatenate([gath[s, p] for s in range(n_tp)], axis=1)
        pre = dot(x, w[...])
        gt = dot(gates_ref[...], x, ((1,), (1,)))
        graw[0, pl.ds(0, heads)] = gt[:heads]
        graw[1, pl.ds(0, heads)] = gt[heads:]
        gd = graw[0, pl.ds(first_head, pad)]
        gb = graw[1, pl.ds(first_head, pad)]
        rate = jnp.zeros((pad, seg), F32)
        bias = jnp.zeros((pad, seg), F32)
        for h in range(nh):
            rate = jnp.where(row_id == h, rate_ref[h], rate)
            bias = jnp.where(row_id == h, bias_ref[h], bias)
        extra = jnp.concatenate([extra_ref[p], jnp.zeros((pad - nh, seg), F32)], axis=0)
        soft = jnp.maximum(gd, 0.0) + jnp.log1p(jnp.exp(-jnp.abs(gd)))
        log_decay = extra - rate * soft
        beta = jax.nn.sigmoid(gb + bias)
        run = dot(log_decay, upper[...], precision=HIGH)
        end = run[:, seg - 1 : seg]
        decs[p] = jnp.broadcast_to(jnp.exp(end), (pad, DV))
        cols = jnp.concatenate(
            [run, beta, beta * jnp.exp(run), jnp.exp(end - run)], axis=0
        ).T
        act = pre * jax.nn.sigmoid(pre)
        lev = level[...]
        strict = lev >= 0
        eye = jnp.where(
            lax.broadcasted_iota(jnp.int32, (seg, seg), 0)
            == lax.broadcasted_iota(jnp.int32, (seg, seg), 1),
            1.0,
            0.0,
        ).astype(F32)
        keys, lower, inv = [], [], []
        for h in range(nh):
            raw = act[:, h * DK : (h + 1) * DK]
            key = raw * lax.rsqrt(jnp.sum(raw * raw, axis=-1, keepdims=True) + EPS)
            kb = key.astype(BF)
            gram = dot(kb, kb, ((1,), (1,)))
            spread = cols[:, h : h + 1] - run[h : h + 1, :]
            weight = jnp.exp(jnp.where(strict, spread, 0.0))
            low = jnp.where(strict, gram * weight * cols[:, pad + h : pad + h + 1], 0.0)
            keys.append(key)
            lower.append(low)
            inv.append(jnp.where(lev == 0, -low, 0.0))
        for step in range(1, levels):
            cuts = [jnp.where(lev == step, low, 0.0) for low in lower]
            full = [(eye + part).astype(BF) for part in inv]
            mids = [dot(cut.astype(BF), f) for cut, f in zip(cuts, full)]
            inv = [
                part - dot(f, mid.astype(BF)) for part, f, mid in zip(inv, full, mids)
            ]
        for h in range(nh):
            value = act[:, width + h * DV : width + (h + 1) * DV]
            side = jnp.concatenate(
                [
                    value * cols[:, pad + h : pad + h + 1],
                    keys[h] * cols[:, 2 * pad + h : 2 * pad + h + 1],
                ],
                axis=1,
            )
            solved = side + dot(inv[h].astype(BF), side.astype(BF))
            late = keys[h] * cols[:, 3 * pad + h : 3 * pad + h + 1]
            late_top = late.astype(BF)
            late_rest = (late - late_top.astype(F32)).astype(BF)
            top = solved.astype(BF)
            rest = (solved[:, :DV] - top[:, :DV].astype(F32)).astype(BF)
            tall = ((0,), (0,))
            both = dot(late_top, top, tall)
            adds[p, h] = (
                both[:, :DV] + dot(late_top, rest, tall) + dot(late_rest, top[:, :DV], tall)
            )
            maps[p, h] = both[:, DV:].astype(BF)

    def unite(p):
        def merge(j, early, late, early_dec, late_dec):
            h = mine + j
            map_0, add_0 = early[0][...], early[1][...]
            map_1, add_1 = late[0][...], late[1][...]
            dec_0 = early_dec[p, pl.ds(h, 1)]
            dec_1 = late_dec[p, pl.ds(h, 1)]
            turn = dot(map_1, jnp.concatenate([map_0, add_0.astype(BF)], axis=1))
            maps[p, h] = (
                dec_1 * map_0.astype(F32) + dec_0 * map_1.astype(F32) - turn[:, :DK]
            ).astype(BF)
            adds[p, h] = dec_1 * add_0 + add_1 - turn[:, DK:]

        @pl.when(has_mine)
        def _():
            for copy in pair_copies(p):
                copy.wait_recv()
            joint_decs[p] = decs[p] * pair_decs[p]
            for first in range(2):

                @pl.when(core == first)
                def _():
                    for j in range(share):
                        own = (maps.at[p, mine + j], adds.at[p, mine + j])
                        got = (pair_maps.at[p, j], pair_adds.at[p, j])
                        if first == 0:
                            merge(j, own, got, decs, pair_decs)
                        else:
                            merge(j, got, own, pair_decs, decs)

    def advance(p):
        @pl.when(chip == 0)
        def _():
            for j in range(share):
                sent[p, j] = adds[p, mine + j].astype(BF)
                chain_copy(p, j).start()

        def moved(j):
            chain_copy(p, j).wait_recv()
            state = came[p, j]
            h = mine + j
            return (
                joint_decs[p, pl.ds(h, 1)] * state.astype(F32)
                + adds[p, h]
                - dot(maps[p, h], state)
            )

        @pl.when(jnp.logical_and(chip > 0, chip < last_chip))
        def _():
            for j in range(share):
                sent[p, j] = moved(j).astype(BF)
                chain_copy(p, j).start()

        @pl.when(chip == last_chip)
        def _():
            for j in range(share):
                state = moved(j).astype(BF)
                final[p, j] = state
                raw = dot(query_heads[mine + j], state)
                norm = (
                    raw
                    * lax.rsqrt(jnp.mean(raw * raw, axis=-1, keepdims=True) + EPS)
                    * gain_ref[...]
                )
                at_p = lax.broadcasted_iota(jnp.int32, norm.shape, 0) == p
                read_buf[j] = jnp.where(at_p, norm, read_buf[j])
            for c in range(chunks):
                owner = p * chunks + c

                @pl.when(owner != sp)
                def _():
                    state_copy(p, c, core).start()

                @pl.when(owner == sp)
                def _():
                    for j in range(share):
                        landing[mine + j] = final[p, j, c * rows : (c + 1) * rows]

    ending = jnp.logical_and(chip == last_chip, has_mine)

    @pl.when(ending)
    def _():
        read_buf[...] = jnp.zeros_like(read_buf)
        for h in range(nh):
            query_heads[h] = query_ref[:, h * DK : (h + 1) * DK]

    lag = 1 + chip

    def body(it, carry):
        if relay:

            @pl.when(it + ahead < prompts)
            def _():
                pass_on(it + ahead)

            @pl.when(it + ahead + early < prompts)
            def _():
                start_direct(it + ahead + early)

        @pl.when(it < prompts)
        def _():
            if relay:
                passed(it, 0).wait_recv()
                passed(it, 1).wait_recv()
            else:

                def take(step, carry):
                    plain(it, step).wait_recv()
                    return carry

                lax.fori_loop(1, n_tp, take, 0)
            work(it)

            @pl.when(has_theirs)
            def _():
                for copy in pair_copies(it):
                    copy.start()

        @pl.when(jnp.logical_and(it >= 1, it < prompts + 1))
        def _():
            unite(it - 1)

        moving = jnp.logical_and(it >= lag, it < prompts + lag)

        @pl.when(jnp.logical_and(moving, has_mine))
        def _():
            advance(it - lag)

        return carry

    lax.fori_loop(0, prompts + last_chip + 1, body, 0)

    @pl.when(ending)
    def _():
        def tell(target, carry):
            @pl.when(target != sp)
            def _():
                read_copy(target, core).start()

            return carry

        lax.fori_loop(0, n_sp, tell, 0)
        for j in range(share):
            read_land[mine + j] = read_buf[j]

    for k in sources:

        @pl.when(sp != 2 * last_chip + k)
        def _():
            state_copy(0, 0, k).wait_recv()
            read_copy(0, k).wait_recv()

    for h in range(nh):
        state_out[:, h * DV : (h + 1) * DV] = landing[h]
        read_out[:, h * DV : (h + 1) * DV] = read_land[h].astype(BF)

    @pl.when(ending)
    def _():
        def told(target, carry):
            @pl.when(target != sp)
            def _():
                read_copy(target, core).wait_send()
                state_copy(target // chunks, lax.rem(target, chunks), core).wait_send()

            return carry

        lax.fori_loop(0, n_sp, told, 0)

    @pl.when(jnp.logical_and(chip < last_chip, has_mine))
    def _():
        def left(index, carry):
            chain_copy(index // share, lax.rem(index, share)).wait_send()
            return carry

        lax.fori_loop(0, prompts * share, left, 0)

    @pl.when(has_theirs)
    def _():
        def lent(index, carry):
            for copy in pair_copies(index):
                copy.wait_send()
            return carry

        lax.fori_loop(0, prompts, lent, 0)

    def freed(index, carry):
        if relay:
            direct(index, 0).wait_send()
            direct(index, 1).wait_send()
            passed(index, 0).wait_send()
            passed(index, 1).wait_send()
        else:
            for step in range(1, n_tp):
                plain(index, step).wait_send()
        return carry

    lax.fori_loop(0, prompts, freed, 0)


def near(
    n_sp,
    n_tp,
    nh,
    x_hbm,
    wk_hbm,
    wv_hbm,
    gates_hbm,
    rate_hbm,
    bias_hbm,
    extra_hbm,
    query_hbm,
    gain_hbm,
    state_out,
    read_out,
    gates_ref,
    rate_ref,
    bias_ref,
    extra_ref,
    query_ref,
    gain_ref,
    gath,
    w,
    gall,
    gsel,
    fixed,
    level,
    upper,
    acc,
    gacc,
    maps,
    adds,
    decs,
    up_out,
    up_in,
    down_out,
    down_in,
    query,
    read_buf,
    read_land,
    local_sem,
    x_sem,
    gsend,
    grecv,
    usend,
    urecv,
    dsend,
    drecv,
    rsend,
    rrecv,
):
    prompts, seg, depth = x_hbm.shape
    width = nh * DK
    heads = gates_ref.shape[0] // 2
    pad = 8
    last = n_sp - 1
    sp = lax.axis_index("sp")
    tp = lax.axis_index("tp")
    core = lax.rem(sp, 2)
    chip = sp // 2
    chips = n_sp // 2
    map_at = 4 * pad
    add_at = map_at + nh * DK
    low_at = add_at + nh * DK

    def prompt_at(t):
        rev = chips - 1 - t // 2
        owner = 0
        k = 1
        while k < chips:
            owner = owner + k * lax.rem(chip // k + rev // k, 2)
            k *= 2
        flip = (2 * (owner - chip) + 1 - core + n_sp - 1) // n_sp
        return 2 * owner + lax.rem(flip + lax.rem(t, 2), 2)

    def x_copy(t):
        p = prompt_at(t)
        return pltpu.make_async_copy(
            x_hbm.at[p], gath.at[tp, p], x_sem.at[min(t, early)]
        )

    early = min(2, prompts)
    for t in range(prompts):
        x_copy(t).start()

    barrier = pltpu.get_barrier_semaphore()
    xn = tp + 1 - 2 * lax.rem(tp, 2)
    yn = tp + 2 - 4 * (tp // 2)
    far = n_tp - 1 - tp

    def greet_sp(step, carry):
        pl.semaphore_signal(barrier, inc=1, device_id={"sp": lax.rem(sp + step, n_sp)})
        return carry

    lax.fori_loop(1, n_sp, greet_sp, 0)
    pl.semaphore_signal(barrier, inc=1, device_id={"tp": xn})
    pl.semaphore_signal(barrier, inc=1, device_id={"tp": yn})
    loads = [
        pltpu.make_async_copy(source, target, local_sem.at[k])
        for k, (source, target) in enumerate(
            (
                (gates_hbm, gates_ref),
                (rate_hbm, rate_ref),
                (bias_hbm, bias_ref),
                (extra_hbm, extra_ref),
                (query_hbm, query_ref),
                (gain_hbm, gain_ref),
                (wk_hbm, w.at[:, pl.ds(0, width)]),
                (wv_hbm, w.at[:, pl.ds(width, nh * DV)]),
            )
        )
    ]
    pl.semaphore_wait(barrier, 2 + n_sp - 1)

    half = seg // 2

    def direct(t, way):
        p = prompt_at(t)
        return pltpu.make_async_remote_copy(
            src_ref=gath.at[tp, p],
            dst_ref=gath.at[tp, p],
            send_sem=gsend.at[0],
            recv_sem=grecv.at[way, t],
            device_id={"tp": xn if way == 0 else yn},
        )

    def passed(t, way):
        p = prompt_at(t)
        source = xn if way == 0 else yn
        part = pl.ds(way * half, half)
        return pltpu.make_async_remote_copy(
            src_ref=gath.at[source, p, part],
            dst_ref=gath.at[source, p, part],
            send_sem=gsend.at[0],
            recv_sem=grecv.at[2, t],
            device_id={"tp": yn if way == 0 else xn},
        )

    def start_direct(t):
        direct(t, 0).start()
        direct(t, 1).start()

    def pass_on(t):
        direct(t, 0).wait_recv()
        passed(t, 0).start()
        direct(t, 1).wait_recv()
        passed(t, 1).start()

    def gathered(t):
        block = gath.at[far, prompt_at(t)]
        pltpu.make_async_remote_copy(
            src_ref=block,
            dst_ref=block,
            send_sem=gsend.at[0],
            recv_sem=grecv.at[2, t],
            device_id={"tp": xn},
        ).wait_recv()

    def up_copy(t, full):
        return pltpu.make_async_remote_copy(
            src_ref=up_out.at[t] if full else up_out.at[t, 0],
            dst_ref=up_in.at[t] if full else up_in.at[t, 0],
            send_sem=usend.at[lax.rem(t, 2)],
            recv_sem=urecv.at[t],
            device_id={"sp": sp + 1},
        )

    def down_copy(t, full):
        part = pl.ds(0, down_out.shape[1] if full else low_at)
        return pltpu.make_async_remote_copy(
            src_ref=down_out.at[t, part],
            dst_ref=down_in.at[t, part],
            send_sem=dsend.at[lax.rem(t, 2)],
            recv_sem=drecv.at[t],
            device_id={"sp": sp - 1},
        )

    def on_core(which, act):
        pl.when(core == which)(lambda: act(True))
        pl.when(core != which)(lambda: act(False))

    def read_copy(target, source):
        return pltpu.make_async_remote_copy(
            src_ref=read_buf,
            dst_ref=read_land.at[source],
            send_sem=rsend.at[0],
            recv_sem=rrecv.at[0],
            device_id={"sp": target},
        )

    def band(source):
        return pl.ds(pl.multiple_of(source * depth, depth), depth)

    levels = 1
    while (1 << levels) < seg:
        levels += 1
    groups = [(k, min(k + 3, levels)) for k in range(1, levels, 3)]
    tile = DK + DV
    near_by = (tp, xn, yn)

    def ahead(t):
        p = prompt_at(t)
        slot = lax.rem(t, 2)
        x = jnp.concatenate([gath[s, p] for s in near_by], axis=1)

        def gate_piece():
            g = jnp.concatenate([gsel[:, band(s)] for s in near_by], axis=1)
            gacc[slot] = dot(g, x, ((1,), (1,)))

        def piece(at):
            def go():
                cols = pl.ds(at * tile, tile)
                side = jnp.concatenate([w[band(s), cols] for s in near_by], axis=0)
                acc[slot, :, cols] = dot(x, side)

            return go

        return [gate_piece] + [piece(at) for at in range(2 * width // tile)]

    def work(t, pieces):
        pieces = list(pieces)

        def fill():
            if pieces:
                pieces.pop(0)()

        p = prompt_at(t)
        slot = lax.rem(t, 2)
        x = gath[far, p]
        gt = gacc[slot] + dot(gsel[:, band(far)], x, ((1,), (1,)))
        key_pre = acc[slot, :, :width] + dot(x, w[band(far), :width])
        value_pre = acc[slot, :, width:] + dot(x, w[band(far), width:])
        gd = gt[:pad]
        gb = gt[pad:]
        extra = jnp.concatenate([extra_ref[p], jnp.zeros((pad - nh, seg), F32)], axis=0)
        soft = jnp.maximum(gd, 0.0) + jnp.log1p(jnp.exp(-jnp.abs(gd)))
        log_decay = extra - fixed[0] * soft
        beta = jax.nn.sigmoid(gb + fixed[1])
        high = log_decay.astype(BF).astype(F32)
        rest = log_decay - high
        mid = rest.astype(BF).astype(F32)
        split = jnp.concatenate([high, mid, rest - mid, jnp.zeros_like(high)], axis=0)
        sums = dot(split.astype(BF), upper[...])
        run = sums[:pad] + sums[pad : 2 * pad] + sums[2 * pad : 3 * pad]
        end = run[:, seg - 1 : seg]
        decs[p] = jnp.broadcast_to(jnp.exp(end), (pad, DV))
        cols = jnp.concatenate(
            [run, beta, beta * jnp.exp(run), jnp.exp(end - run)], axis=0
        ).T
        lev = level[...]
        strict = lev >= 0
        eye = jnp.where(
            lax.broadcasted_iota(jnp.int32, (seg, seg), 0)
            == lax.broadcasted_iota(jnp.int32, (seg, seg), 1),
            1.0,
            0.0,
        ).astype(F32)
        hs = range(nh)
        keys, grams = [], []
        for h in hs:
            pre = key_pre[:, h * DK : (h + 1) * DK]
            raw = pre * jax.nn.sigmoid(pre)
            key = raw * lax.rsqrt(jnp.sum(raw * raw, axis=-1, keepdims=True) + EPS)
            kb = key.astype(BF)
            keys.append(key)
            grams.append(dot(kb, kb, ((1,), (1,))))
        fill()
        fill()
        lower, inv = [], []
        for h in hs:
            spread = cols[:, h : h + 1] - run[h : h + 1, :]
            weight = jnp.exp(jnp.where(strict, spread, 0.0))
            low = jnp.where(strict, grams[h] * weight * cols[:, pad + h : pad + h + 1], 0.0)
            lower.append(low)
            inv.append(eye - jnp.where(lev == 0, low, 0.0))

        def merge(first, until):
            inside = jnp.logical_and(lev >= first, lev < until)
            cuts = [jnp.where(inside, low, 0.0).astype(BF) for low in lower]
            return [dot(f.astype(BF), cut).astype(BF) for f, cut in zip(inv, cuts)]

        for first, until in groups[:-1]:
            steps = merge(first, until)
            fill()
            inv = [f - dot(e, f.astype(BF)) for e, f in zip(steps, inv)]
            for _ in range(first + 1, until):
                steps = [dot(e, e).astype(BF) for e in steps]
                fill()
                inv = [f + dot(e, f.astype(BF)) for e, f in zip(steps, inv)]
        sides = []
        for h in hs:
            pre = value_pre[:, h * DV : (h + 1) * DV]
            value = pre * jax.nn.sigmoid(pre)
            sides.append(
                jnp.concatenate(
                    [
                        value * cols[:, pad + h : pad + h + 1],
                        keys[h] * cols[:, 2 * pad + h : 2 * pad + h + 1],
                    ],
                    axis=1,
                )
            )
        first, until = groups[-1]
        steps = merge(first, until)
        sides = [
            side + dot((f - eye).astype(BF), side.astype(BF)) for f, side in zip(inv, sides)
        ]
        fill()
        sides = [side - dot(e, side.astype(BF)) for e, side in zip(steps, sides)]
        for _ in range(first + 1, until):
            steps = [dot(e, e).astype(BF) for e in steps]
            fill()
            sides = [side + dot(e, side.astype(BF)) for e, side in zip(steps, sides)]
        while pieces:
            fill()
        tall = ((0,), (0,))
        for h in hs:
            late = keys[h] * cols[:, 3 * pad + h : 3 * pad + h + 1]
            late_top = late.astype(BF)
            late_rest = (late - late_top.astype(F32)).astype(BF)
            top = sides[h].astype(BF)
            rest = (sides[h][:, :DV] - top[:, :DV].astype(F32)).astype(BF)
            both = dot(late_top, top, tall)
            adds[p, h] = (
                both[:, :DV] + dot(late_top, rest, tall) + dot(late_rest, top[:, :DV], tall)
            )
            maps[p, h] = both[:, DV:].astype(BF)

    def moved(at, p, h):
        top = up_in[at, 0, h]
        state = top.astype(F32) + up_in[at, 1, h].astype(F32)
        return decs[p, pl.ds(h, 1)] * state + adds[p, h] - dot(maps[p, h], top)

    def go_up(t, p, fresh):
        for h in range(nh):
            state = adds[p, h] if fresh else moved(t - 1, p, h)
            top = state.astype(BF)
            up_out[t, 0, h] = top
            up_out[t, 1, h] = (state - top.astype(F32)).astype(BF)

    def later(at):
        part = down_in[at, pl.ds(0, map_at)].astype(F32)
        return part[:pad] + part[pad : 2 * pad] + part[2 * pad : 3 * pad]

    def rows(first, h):
        return pl.ds(first + h * DK, DK)

    def total(at, h):
        top = down_in[at, rows(add_at, h)].astype(F32)
        return top + down_in[at, rows(low_at, h)].astype(F32)

    def go_down(t, p, fresh):
        own = decs[p]
        dec = None if fresh else later(t - 1)
        for h in range(nh):
            add = adds[p, h]
            if fresh:
                down_out[t, rows(map_at, h)] = maps[p, h]
            else:
                late = down_in[t - 1, rows(map_at, h)]
                early = maps[p, h]
                turn = dot(late, jnp.concatenate([early, add.astype(BF)], axis=1))
                add = dec[h : h + 1] * add + total(t - 1, h) - turn[:, DK:]
                both = dec[h : h + 1] * early.astype(F32) + own[h : h + 1] * late.astype(F32)
                down_out[t, rows(map_at, h)] = (both - turn[:, :DK]).astype(BF)
            top = add.astype(BF)
            down_out[t, rows(add_at, h)] = top
            down_out[t, rows(low_at, h)] = (add - top.astype(F32)).astype(BF)
        dec = own if fresh else own * dec
        high = dec.astype(BF).astype(F32)
        rest = dec - high
        mid = rest.astype(BF).astype(F32)
        split = jnp.concatenate([high, mid, rest - mid, jnp.zeros_like(high)], axis=0)
        down_out[t, pl.ds(0, map_at)] = split.astype(BF)

    def wait_up(t):
        on_core(1, lambda full: up_copy(t, full).wait_recv())

    def wait_down(t):
        on_core(0, lambda full: down_copy(t, full).wait_recv())

    def chain_up(t):
        rev = last - t

        @pl.when(sp + rev <= last)
        def _():
            @pl.when(sp == 0)
            def _():
                go_up(t, rev, True)

            @pl.when(sp > 0)
            def _():
                wait_up(t - 1)
                go_up(t, sp + rev, False)

            @pl.when(sp + rev + 2 <= last)
            def _():
                on_core(0, lambda full: up_copy(t - 2, full).wait_send())

            on_core(0, lambda full: up_copy(t, full).start())

    def chain_down(t):
        rev = last - t

        @pl.when(sp >= rev)
        def _():
            @pl.when(sp == last)
            def _():
                go_down(t, last - rev, True)

            @pl.when(sp < last)
            def _():
                wait_down(t - 1)
                go_down(t, sp - rev, False)

            @pl.when(sp >= rev + 2)
            def _():
                on_core(1, lambda full: down_copy(t - 2, full).wait_send())

            on_core(1, lambda full: down_copy(t, full).start())

    def before(t):
        pl.when(core == 0)(lambda: chain_down(t))
        pl.when(core == 1)(lambda: chain_up(t))

    def after(t):
        pl.when(core == 0)(lambda: chain_up(t))
        pl.when(core == 1)(lambda: chain_down(t))

    def close(below, above):
        at = last - 1
        dec = later(at) if above else None
        for h in range(nh):
            state = moved(at, sp, h) if below else adds[sp, h]
            if above:
                state = (
                    dec[h : h + 1] * state
                    + total(at, h)
                    - dot(down_in[at, rows(map_at, h)], state.astype(BF))
                )
            cached = state.astype(BF)
            state_out[:, h * DV : (h + 1) * DV] = cached
            raw = dot(query[h].astype(BF), cached)
            norm = (
                raw
                * lax.rsqrt(jnp.mean(raw * raw, axis=-1, keepdims=True) + EPS)
                * gain_ref[...]
            )
            read_buf[pl.ds(h, 1)] = norm[:1]

    for t in range(early):
        x_copy(t).wait()
        start_direct(t)
    for load in loads:
        load.start()
    if early < prompts:
        others = pl.ds(0, prompts - early)
        pltpu.make_async_copy(
            x_hbm.at[others], gath.at[tp, others], x_sem.at[early]
        ).wait()
    for load in loads[:6]:
        load.wait()

    r_id = lax.broadcasted_iota(jnp.int32, (seg, seg), 0)
    c_id = lax.broadcasted_iota(jnp.int32, (seg, seg), 1)
    lev = jnp.zeros((seg, seg), jnp.int32)
    k = 1
    while (1 << k) < seg:
        lev = jnp.where((r_id >> k) != (c_id >> k), k, lev)
        k += 1
    level[...] = jnp.where(r_id > c_id, lev, -1)
    upper[...] = jnp.where(r_id <= c_id, 1.0, 0.0).astype(BF)

    row_id = lax.broadcasted_iota(jnp.int32, (pad, seg), 0)
    rate = jnp.zeros((pad, seg), F32)
    bias = jnp.zeros((pad, seg), F32)
    for h in range(nh):
        rate = jnp.where(row_id == h, rate_ref[h], rate)
        bias = jnp.where(row_id == h, bias_ref[h], bias)
    fixed[0] = rate
    fixed[1] = bias
    for at in range(n_tp * depth // 128):
        part = gates_ref[:, at * 128 : (at + 1) * 128].astype(F32)
        gall[at, pl.ds(0, heads)] = part[:heads]
        gall[at, pl.ds(heads, heads)] = part[heads:]
        gall[at, pl.ds(2 * heads, pad)] = jnp.zeros((pad, 128), F32)
        picked = [gall[at, pl.ds(tp * nh + k * heads, pad)] for k in range(2)]
        gsel[:, at * 128 : (at + 1) * 128] = jnp.concatenate(picked, axis=0).astype(BF)
    every = query_ref[...].astype(F32)
    mine = lax.broadcasted_iota(jnp.int32, every.shape, 0) == sp
    asked = jnp.sum(jnp.where(mine, every, 0.0), axis=0, keepdims=True)
    for h in range(nh):
        query[h] = jnp.broadcast_to(asked[:, h * DK : (h + 1) * DK], (pad, DK))
    read_buf[...] = jnp.zeros_like(read_buf)

    @pl.when(core == 0)
    def _():
        up_in[:, 1] = jnp.zeros((n_sp - 1, nh, DK, DV), BF)

    @pl.when(core == 1)
    def _():
        down_in[:, pl.ds(low_at, nh * DK)] = jnp.zeros((n_sp - 1, nh * DK, DV), BF)


    pass_on(0)
    if early < prompts:
        start_direct(early)
    for load in loads[6:]:
        load.wait()
    for go in ahead(0):
        go()

    def body(t, carry):
        pass_on(t + 1)

        @pl.when(t + 1 + early < prompts)
        def _():
            start_direct(t + 1 + early)

        gathered(t)
        before(t)
        work(t, ahead(t + 1))
        after(t)
        return carry

    lax.fori_loop(0, last, body, 0)
    gathered(last)
    work(last, [])

    @pl.when(sp > 0)
    def _():
        wait_up(last - 1)

    @pl.when(sp < last)
    def _():
        wait_down(last - 1)

    @pl.when(sp == 0)
    def _():
        close(False, True)

    @pl.when(jnp.logical_and(sp > 0, sp < last))
    def _():
        close(True, True)

    @pl.when(sp == last)
    def _():
        close(True, False)

    def tell(step, carry):
        target = lax.rem(sp + step, n_sp)
        read_copy(target, sp).start()
        return carry

    lax.fori_loop(1, n_sp, tell, 0)
    read_land[sp] = read_buf[...]

    block = gath.at[pl.ds(0, n_tp - 1)]
    pltpu.make_async_remote_copy(
        src_ref=block,
        dst_ref=block,
        send_sem=gsend.at[0],
        recv_sem=grecv.at[2, 0],
        device_id={"tp": xn},
    ).wait_send()

    for back in range(1, min(last, 2) + 1):

        @pl.when(sp + back <= last)
        def _():
            on_core(0, lambda full: up_copy(last - back, full).wait_send())

        @pl.when(sp >= back)
        def _():
            on_core(1, lambda full: down_copy(last - back, full).wait_send())

    others = read_land.at[pl.ds(0, last)]
    reads = pltpu.make_async_remote_copy(
        src_ref=others,
        dst_ref=others,
        send_sem=rsend.at[0],
        recv_sem=rrecv.at[0],
        device_id={"sp": lax.rem(sp + 1, n_sp)},
    )
    reads.wait_send()
    reads.wait_recv()
    for h in range(nh):
        read_out[:, h * DV : (h + 1) * DV] = read_land[:, h].astype(BF)


def close_by(n_sp, n_tp, prompts, seg, rows, nh):
    even = n_sp >= 2 and n_sp & (n_sp - 1) == 0 and seg & (seg - 1) == 0
    return even and n_tp == 4 and prompts == n_sp and rows == DK and nh <= 8 and seg >= 8


def shards(
    n_sp,
    n_tp,
    layer_input,
    w_key,
    w_value,
    w_gates,
    decay_rate,
    beta_bias,
    log_decay_extra,
    new_query,
    read_gain,
):
    prompts, seg, depth = layer_input.shape
    whole_depth, width = w_key.shape
    nh = width // DK
    heads = w_gates.shape[2]
    rows = prompts * DK // n_sp
    share = max(nh // 2, 1)
    gates = jnp.swapaxes(w_gates, 1, 2).reshape(2 * heads, whole_depth)
    vmem = pl.BlockSpec(memory_space=pltpu.VMEM)
    smem = pl.BlockSpec(memory_space=pltpu.SMEM)
    hbm = pl.BlockSpec(memory_space=pl.ANY)
    dma = pltpu.SemaphoreType.DMA
    if close_by(n_sp, n_tp, prompts, seg, rows, nh):
        hops = n_sp - 1
        return pl.pallas_call(
            functools.partial(near, n_sp, n_tp, nh),
            out_shape=(
                pltpu.VMEM((rows, nh * DV), BF),
                pltpu.VMEM((prompts, nh * DV), BF),
            ),
            in_specs=[hbm] * 9,
            out_specs=(vmem, vmem),
            scratch_shapes=[
                pltpu.VMEM((2 * heads, whole_depth), BF),
                pltpu.SMEM((nh,), F32),
                pltpu.SMEM((nh,), F32),
                pltpu.VMEM((prompts, nh, seg), F32),
                pltpu.VMEM((prompts, nh * DK), BF),
                pltpu.VMEM((1, DV), F32),
                pltpu.VMEM((n_tp, prompts, seg, depth), BF),
                pltpu.VMEM((whole_depth, nh * (DK + DV)), BF),
                pltpu.VMEM((whole_depth // 128, 2 * heads + 8, 128), F32),
                pltpu.VMEM((16, whole_depth), BF),
                pltpu.VMEM((2, 8, seg), F32),
                pltpu.VMEM((seg, seg), jnp.int32),
                pltpu.VMEM((seg, seg), BF),
                pltpu.VMEM((2, seg, nh * (DK + DV)), F32),
                pltpu.VMEM((2, 16, seg), F32),
                pltpu.VMEM((prompts, nh, DK, DK), BF),
                pltpu.VMEM((prompts, nh, DK, DV), F32),
                pltpu.VMEM((prompts, 8, DV), F32),
                pltpu.VMEM((hops, 2, nh, DK, DV), BF),
                pltpu.VMEM((hops, 2, nh, DK, DV), BF),
                pltpu.VMEM((hops, 32 + 3 * nh * DK, DV), BF),
                pltpu.VMEM((hops, 32 + 3 * nh * DK, DV), BF),
                pltpu.VMEM((nh, 8, DK), F32),
                pltpu.VMEM((8, DV), F32),
                pltpu.VMEM((prompts, 8, DV), F32),
                dma((8,)),
                dma((min(2, prompts) + 1,)),
                dma((1,)),
                dma((3, prompts)),
                dma((2,)),
                dma((hops,)),
                dma((2,)),
                dma((hops,)),
                dma((1,)),
                dma((1,)),
            ],
            compiler_params=pltpu.CompilerParams(
                collective_id=0, has_side_effects=True, vmem_limit_bytes=56 * 1024 * 1024
            ),
        )(
            layer_input,
            w_key,
            w_value,
            gates,
            decay_rate,
            beta_bias,
            log_decay_extra,
            new_query,
            read_gain.reshape(1, DV),
        )
    return pl.pallas_call(
        functools.partial(kernel, n_sp, n_tp, nh, rows),
        out_shape=(
            jax.ShapeDtypeStruct((rows, nh * DV), BF),
            jax.ShapeDtypeStruct((prompts, nh * DV), BF),
        ),
        in_specs=[hbm, hbm, hbm, vmem, smem, smem, vmem, vmem, vmem],
        out_specs=(vmem, vmem),
        scratch_shapes=[
            pltpu.VMEM((n_tp, prompts, seg, depth), BF),
            pltpu.VMEM((whole_depth, nh * (DK + DV)), BF),
            pltpu.VMEM((2, heads + 8, seg), F32),
            pltpu.VMEM((seg, seg), jnp.int32),
            pltpu.VMEM((seg, seg), F32),
            pltpu.VMEM((prompts, nh, DK, DK), BF),
            pltpu.VMEM((prompts, nh, DK, DV), F32),
            pltpu.VMEM((prompts, 8, DV), F32),
            pltpu.VMEM((prompts, share, DK, DK), BF),
            pltpu.VMEM((prompts, share, DK, DV), F32),
            pltpu.VMEM((prompts, 8, DV), F32),
            pltpu.VMEM((prompts, 8, DV), F32),
            pltpu.VMEM((prompts, share, DK, DV), BF),
            pltpu.VMEM((prompts, share, DK, DV), BF),
            pltpu.VMEM((prompts, share, DK, DV), BF),
            pltpu.VMEM((nh, rows, DV), BF),
            pltpu.VMEM((share, prompts, DV), F32),
            pltpu.VMEM((nh, prompts, DV), F32),
            pltpu.VMEM((nh, prompts, DK), BF),
            dma((3,)),
            dma((max(n_tp, 4), prompts)),
            dma((max(n_tp, 4), prompts)),
            dma((3, prompts)),
            dma((3, prompts)),
            dma((prompts, share)),
            dma((prompts, share)),
            dma((prompts, DK // rows)),
            dma((2,)),
            dma((n_sp,)),
            dma((2,)),
        ],
        compiler_params=pltpu.CompilerParams(
            collective_id=0, has_side_effects=True, vmem_limit_bytes=56 * 1024 * 1024
        ),
    )(
        layer_input,
        w_key,
        w_value,
        gates,
        decay_rate,
        beta_bias,
        log_decay_extra,
        new_query,
        read_gain.reshape(1, DV),
    )


def solution(mesh):
    return jax.shard_map(
        functools.partial(shards, mesh.shape["sp"], mesh.shape["tp"]),
        mesh=mesh,
        in_specs=(
            P(None, "sp", "tp"),
            P(None, "tp"),
            P(None, "tp"),
            P(),
            P("tp"),
            P("tp"),
            P(None, "tp", "sp"),
            P(None, "tp"),
            P(),
        ),
        out_specs=(P("sp", "tp"), P(None, "tp")),
        check_vma=False,
    )
```

```python
import functools

import jax
import jax.numpy as jnp
from jax import lax
from jax.experimental import pallas as pl
from jax.experimental.pallas import tpu as pltpu
from jax.sharding import PartitionSpec as P

DK = 128
DV = 128
EPS = 1e-06
HIGH = lax.Precision.HIGHEST
BF = jnp.bfloat16
F32 = jnp.float32


def dot(left, right, dims=((1,), (0,)), precision=None):
    return lax.dot_general(
        left, right, (dims, ((), ())), precision=precision, preferred_element_type=F32
    )


def kernel(
    n_sp,
    n_tp,
    nh,
    rows,
    x_hbm,
    wk_hbm,
    wv_hbm,
    gates_ref,
    rate_ref,
    bias_ref,
    extra_ref,
    query_ref,
    gain_ref,
    state_out,
    read_out,
    gath,
    w,
    graw,
    level,
    upper,
    maps,
    adds,
    decs,
    pair_maps,
    pair_adds,
    pair_decs,
    joint_decs,
    came,
    sent,
    final,
    landing,
    read_buf,
    read_land,
    query_heads,
    local_sem,
    gsend,
    grecv,
    psend,
    precv,
    csend,
    crecv,
    ssend,
    srecv,
    rsend,
    rrecv,
):
    prompts, seg, depth = x_hbm.shape
    width = nh * DK
    heads = gates_ref.shape[0] // 2
    sp = lax.axis_index("sp")
    tp = lax.axis_index("tp")
    core = lax.rem(sp, 2)
    other = 1 - core
    chip = sp // 2
    last_chip = n_sp // 2 - 1
    share = max(nh // 2, 1)
    mine = core * share
    theirs = other * share
    has_mine = mine < nh
    has_theirs = theirs < nh
    sources = [k for k in range(2) if k * share < nh]
    chunks = DK // rows
    relay = n_tp == 4

    x_copy = pltpu.make_async_copy(x_hbm, gath.at[tp], local_sem.at[0])
    x_copy.start()
    wk_copy = pltpu.make_async_copy(wk_hbm, w.at[:, pl.ds(0, width)], local_sem.at[1])
    wv_copy = pltpu.make_async_copy(wv_hbm, w.at[:, pl.ds(width, nh * DV)], local_sem.at[2])
    wk_copy.start()
    wv_copy.start()

    barrier = pltpu.get_barrier_semaphore()

    def greet_tp(step, carry):
        pl.semaphore_signal(barrier, inc=1, device_id={"tp": lax.rem(tp + step, n_tp)})
        return carry

    def greet_sp(step, carry):
        pl.semaphore_signal(barrier, inc=1, device_id={"sp": lax.rem(sp + step, n_sp)})
        return carry

    lax.fori_loop(1, n_tp, greet_tp, 0)
    lax.fori_loop(1, n_sp, greet_sp, 0)
    r_id = lax.broadcasted_iota(jnp.int32, (seg, seg), 0)
    c_id = lax.broadcasted_iota(jnp.int32, (seg, seg), 1)
    lev = jnp.zeros((seg, seg), jnp.int32)
    k = 1
    while (1 << k) < seg:
        lev = jnp.where((r_id >> k) != (c_id >> k), k, lev)
        k += 1
    levels = k
    level[...] = jnp.where(r_id > c_id, lev, -1)
    upper[...] = jnp.where(r_id <= c_id, 1.0, 0.0).astype(F32)
    graw[...] = jnp.zeros_like(graw)
    pl.semaphore_wait(barrier, n_tp - 1 + n_sp - 1)
    x_copy.wait()

    xn = tp + 1 - 2 * lax.rem(tp, 2)
    yn = tp + 2 - 4 * (tp // 2)
    half = seg // 2

    def direct(p, way):
        target = xn if way == 0 else yn
        return pltpu.make_async_remote_copy(
            src_ref=gath.at[tp, p],
            dst_ref=gath.at[tp, p],
            send_sem=gsend.at[way, p],
            recv_sem=grecv.at[way, p],
            device_id={"tp": target},
        )

    def passed(p, way):
        source = xn if way == 0 else yn
        target = yn if way == 0 else xn
        part = pl.ds(way * half, half)
        return pltpu.make_async_remote_copy(
            src_ref=gath.at[source, p, part],
            dst_ref=gath.at[source, p, part],
            send_sem=gsend.at[2 + way, p],
            recv_sem=grecv.at[2 + way, p],
            device_id={"tp": target},
        )

    def plain(p, step):
        return pltpu.make_async_remote_copy(
            src_ref=gath.at[tp, p],
            dst_ref=gath.at[tp, p],
            send_sem=gsend.at[step, p],
            recv_sem=grecv.at[step, p],
            device_id={"tp": lax.rem(tp + step, n_tp)},
        )

    def start_direct(p):
        direct(p, 0).start()
        direct(p, 1).start()

    def pass_on(p):
        direct(p, 0).wait_recv()
        passed(p, 0).start()
        direct(p, 1).wait_recv()
        passed(p, 1).start()

    early = min(2, prompts)
    ahead = min(1, prompts)
    if relay:
        for p in range(early):
            start_direct(p)
        for p in range(ahead):
            pass_on(p)
            if early + p < prompts:
                start_direct(early + p)
    else:

        def start_plain(index, carry):
            plain(index // (n_tp - 1), lax.rem(index, n_tp - 1) + 1).start()
            return carry

        lax.fori_loop(0, prompts * (n_tp - 1), start_plain, 0)
    wk_copy.wait()
    wv_copy.wait()

    def pair_copies(p):
        pairs = (
            (maps.at[p, pl.ds(theirs, share)], pair_maps.at[p]),
            (adds.at[p, pl.ds(theirs, share)], pair_adds.at[p]),
            (decs.at[p], pair_decs.at[p]),
        )
        return [
            pltpu.make_async_remote_copy(
                src_ref=source,
                dst_ref=target,
                send_sem=psend.at[i, p],
                recv_sem=precv.at[i, p],
                device_id={"sp": sp + 1 - 2 * core},
            )
            for i, (source, target) in enumerate(pairs)
        ]

    def chain_copy(p, j):
        return pltpu.make_async_remote_copy(
            src_ref=sent.at[p, j],
            dst_ref=came.at[p, j],
            send_sem=csend.at[p, j],
            recv_sem=crecv.at[p, j],
            device_id={"sp": lax.rem(sp + 2, n_sp)},
        )

    def state_copy(p, c, slot):
        return pltpu.make_async_remote_copy(
            src_ref=final.at[p, :, pl.ds(c * rows, rows)],
            dst_ref=landing.at[pl.ds(slot * share, share)],
            send_sem=ssend.at[p, c],
            recv_sem=srecv.at[slot],
            device_id={"sp": p * chunks + c},
        )

    def read_copy(target, slot):
        return pltpu.make_async_remote_copy(
            src_ref=read_buf,
            dst_ref=read_land.at[pl.ds(slot * share, share)],
            send_sem=rsend.at[target],
            recv_sem=rrecv.at[slot],
            device_id={"sp": target},
        )

    first_head = tp * nh
    pad = 8
    row_id = lax.broadcasted_iota(jnp.int32, (pad, seg), 0)

    def work(p):
        x = jnp.concatenate([gath[s, p] for s in range(n_tp)], axis=1)
        pre = dot(x, w[...])
        gt = dot(gates_ref[...], x, ((1,), (1,)))
        graw[0, pl.ds(0, heads)] = gt[:heads]
        graw[1, pl.ds(0, heads)] = gt[heads:]
        gd = graw[0, pl.ds(first_head, pad)]
        gb = graw[1, pl.ds(first_head, pad)]
        rate = jnp.zeros((pad, seg), F32)
        bias = jnp.zeros((pad, seg), F32)
        for h in range(nh):
            rate = jnp.where(row_id == h, rate_ref[h], rate)
            bias = jnp.where(row_id == h, bias_ref[h], bias)
        extra = jnp.concatenate([extra_ref[p], jnp.zeros((pad - nh, seg), F32)], axis=0)
        soft = jnp.maximum(gd, 0.0) + jnp.log1p(jnp.exp(-jnp.abs(gd)))
        log_decay = extra - rate * soft
        beta = jax.nn.sigmoid(gb + bias)
        run = dot(log_decay, upper[...], precision=HIGH)
        end = run[:, seg - 1 : seg]
        decs[p] = jnp.broadcast_to(jnp.exp(end), (pad, DV))
        cols = jnp.concatenate(
            [run, beta, beta * jnp.exp(run), jnp.exp(end - run)], axis=0
        ).T
        act = pre * jax.nn.sigmoid(pre)
        lev = level[...]
        strict = lev >= 0
        eye = jnp.where(
            lax.broadcasted_iota(jnp.int32, (seg, seg), 0)
            == lax.broadcasted_iota(jnp.int32, (seg, seg), 1),
            1.0,
            0.0,
        ).astype(F32)
        keys, lower, inv = [], [], []
        for h in range(nh):
            raw = act[:, h * DK : (h + 1) * DK]
            key = raw * lax.rsqrt(jnp.sum(raw * raw, axis=-1, keepdims=True) + EPS)
            kb = key.astype(BF)
            gram = dot(kb, kb, ((1,), (1,)))
            spread = cols[:, h : h + 1] - run[h : h + 1, :]
            weight = jnp.exp(jnp.where(strict, spread, 0.0))
            low = jnp.where(strict, gram * weight * cols[:, pad + h : pad + h + 1], 0.0)
            keys.append(key)
            lower.append(low)
            inv.append(jnp.where(lev == 0, -low, 0.0))
        for step in range(1, levels):
            cuts = [jnp.where(lev == step, low, 0.0) for low in lower]
            full = [(eye + part).astype(BF) for part in inv]
            mids = [dot(cut.astype(BF), f) for cut, f in zip(cuts, full)]
            inv = [
                part - dot(f, mid.astype(BF)) for part, f, mid in zip(inv, full, mids)
            ]
        for h in range(nh):
            value = act[:, width + h * DV : width + (h + 1) * DV]
            side = jnp.concatenate(
                [
                    value * cols[:, pad + h : pad + h + 1],
                    keys[h] * cols[:, 2 * pad + h : 2 * pad + h + 1],
                ],
                axis=1,
            )
            solved = side + dot(inv[h].astype(BF), side.astype(BF))
            late = keys[h] * cols[:, 3 * pad + h : 3 * pad + h + 1]
            late_top = late.astype(BF)
            late_rest = (late - late_top.astype(F32)).astype(BF)
            top = solved.astype(BF)
            rest = (solved[:, :DV] - top[:, :DV].astype(F32)).astype(BF)
            tall = ((0,), (0,))
            both = dot(late_top, top, tall)
            adds[p, h] = (
                both[:, :DV] + dot(late_top, rest, tall) + dot(late_rest, top[:, :DV], tall)
            )
            maps[p, h] = both[:, DV:].astype(BF)

    def unite(p):
        def merge(j, early, late, early_dec, late_dec):
            h = mine + j
            map_0, add_0 = early[0][...], early[1][...]
            map_1, add_1 = late[0][...], late[1][...]
            dec_0 = early_dec[p, pl.ds(h, 1)]
            dec_1 = late_dec[p, pl.ds(h, 1)]
            turn = dot(map_1, jnp.concatenate([map_0, add_0.astype(BF)], axis=1))
            maps[p, h] = (
                dec_1 * map_0.astype(F32) + dec_0 * map_1.astype(F32) - turn[:, :DK]
            ).astype(BF)
            adds[p, h] = dec_1 * add_0 + add_1 - turn[:, DK:]

        @pl.when(has_mine)
        def _():
            for copy in pair_copies(p):
                copy.wait_recv()
            joint_decs[p] = decs[p] * pair_decs[p]
            for first in range(2):

                @pl.when(core == first)
                def _():
                    for j in range(share):
                        own = (maps.at[p, mine + j], adds.at[p, mine + j])
                        got = (pair_maps.at[p, j], pair_adds.at[p, j])
                        if first == 0:
                            merge(j, own, got, decs, pair_decs)
                        else:
                            merge(j, got, own, pair_decs, decs)

    def advance(p):
        @pl.when(chip == 0)
        def _():
            for j in range(share):
                sent[p, j] = adds[p, mine + j].astype(BF)
                chain_copy(p, j).start()

        def moved(j):
            chain_copy(p, j).wait_recv()
            state = came[p, j]
            h = mine + j
            return (
                joint_decs[p, pl.ds(h, 1)] * state.astype(F32)
                + adds[p, h]
                - dot(maps[p, h], state)
            )

        @pl.when(jnp.logical_and(chip > 0, chip < last_chip))
        def _():
            for j in range(share):
                sent[p, j] = moved(j).astype(BF)
                chain_copy(p, j).start()

        @pl.when(chip == last_chip)
        def _():
            for j in range(share):
                state = moved(j).astype(BF)
                final[p, j] = state
                raw = dot(query_heads[mine + j], state)
                norm = (
                    raw
                    * lax.rsqrt(jnp.mean(raw * raw, axis=-1, keepdims=True) + EPS)
                    * gain_ref[...]
                )
                at_p = lax.broadcasted_iota(jnp.int32, norm.shape, 0) == p
                read_buf[j] = jnp.where(at_p, norm, read_buf[j])
            for c in range(chunks):
                owner = p * chunks + c

                @pl.when(owner != sp)
                def _():
                    state_copy(p, c, core).start()

                @pl.when(owner == sp)
                def _():
                    for j in range(share):
                        landing[mine + j] = final[p, j, c * rows : (c + 1) * rows]

    ending = jnp.logical_and(chip == last_chip, has_mine)

    @pl.when(ending)
    def _():
        read_buf[...] = jnp.zeros_like(read_buf)
        for h in range(nh):
            query_heads[h] = query_ref[:, h * DK : (h + 1) * DK]

    lag = 1 + chip

    def body(it, carry):
        if relay:

            @pl.when(it + ahead < prompts)
            def _():
                pass_on(it + ahead)

            @pl.when(it + ahead + early < prompts)
            def _():
                start_direct(it + ahead + early)

        @pl.when(it < prompts)
        def _():
            if relay:
                passed(it, 0).wait_recv()
                passed(it, 1).wait_recv()
            else:

                def take(step, carry):
                    plain(it, step).wait_recv()
                    return carry

                lax.fori_loop(1, n_tp, take, 0)
            work(it)

            @pl.when(has_theirs)
            def _():
                for copy in pair_copies(it):
                    copy.start()

        @pl.when(jnp.logical_and(it >= 1, it < prompts + 1))
        def _():
            unite(it - 1)

        moving = jnp.logical_and(it >= lag, it < prompts + lag)

        @pl.when(jnp.logical_and(moving, has_mine))
        def _():
            advance(it - lag)

        return carry

    lax.fori_loop(0, prompts + last_chip + 1, body, 0)

    @pl.when(ending)
    def _():
        def tell(target, carry):
            @pl.when(target != sp)
            def _():
                read_copy(target, core).start()

            return carry

        lax.fori_loop(0, n_sp, tell, 0)
        for j in range(share):
            read_land[mine + j] = read_buf[j]

    for k in sources:

        @pl.when(sp != 2 * last_chip + k)
        def _():
            state_copy(0, 0, k).wait_recv()
            read_copy(0, k).wait_recv()

    for h in range(nh):
        state_out[:, h * DV : (h + 1) * DV] = landing[h]
        read_out[:, h * DV : (h + 1) * DV] = read_land[h].astype(BF)

    @pl.when(ending)
    def _():
        def told(target, carry):
            @pl.when(target != sp)
            def _():
                read_copy(target, core).wait_send()
                state_copy(target // chunks, lax.rem(target, chunks), core).wait_send()

            return carry

        lax.fori_loop(0, n_sp, told, 0)

    @pl.when(jnp.logical_and(chip < last_chip, has_mine))
    def _():
        def left(index, carry):
            chain_copy(index // share, lax.rem(index, share)).wait_send()
            return carry

        lax.fori_loop(0, prompts * share, left, 0)

    @pl.when(has_theirs)
    def _():
        def lent(index, carry):
            for copy in pair_copies(index):
                copy.wait_send()
            return carry

        lax.fori_loop(0, prompts, lent, 0)

    def freed(index, carry):
        if relay:
            direct(index, 0).wait_send()
            direct(index, 1).wait_send()
            passed(index, 0).wait_send()
            passed(index, 1).wait_send()
        else:
            for step in range(1, n_tp):
                plain(index, step).wait_send()
        return carry

    lax.fori_loop(0, prompts, freed, 0)


def near(
    n_sp,
    n_tp,
    nh,
    x_hbm,
    wk_hbm,
    wv_hbm,
    gates_hbm,
    rate_hbm,
    bias_hbm,
    extra_hbm,
    query_hbm,
    gain_hbm,
    state_out,
    read_out,
    gates_ref,
    rate_ref,
    bias_ref,
    extra_ref,
    query_ref,
    gain_ref,
    gath,
    w,
    gall,
    gsel,
    fixed,
    level,
    upper,
    acc,
    gacc,
    maps,
    adds,
    decs,
    up_out,
    up_in,
    down_out,
    down_in,
    query,
    read_buf,
    read_land,
    local_sem,
    x_sem,
    gsend,
    grecv,
    usend,
    urecv,
    dsend,
    drecv,
    rsend,
    rrecv,
):
    prompts, seg, depth = x_hbm.shape
    width = nh * DK
    heads = gates_ref.shape[0] // 2
    pad = 8
    last = n_sp - 1
    sp = lax.axis_index("sp")
    tp = lax.axis_index("tp")
    core = lax.rem(sp, 2)
    chip = sp // 2
    chips = n_sp // 2
    map_at = 4 * pad
    add_at = map_at + nh * DK
    low_at = add_at + nh * DK

    def prompt_at(t):
        rev = chips - 1 - t // 2
        owner = 0
        k = 1
        while k < chips:
            owner = owner + k * lax.rem(chip // k + rev // k, 2)
            k *= 2
        flip = (2 * (owner - chip) + 1 - core + n_sp - 1) // n_sp
        return 2 * owner + lax.rem(flip + lax.rem(t, 2), 2)

    def x_copy(t):
        p = prompt_at(t)
        return pltpu.make_async_copy(
            x_hbm.at[p], gath.at[tp, p], x_sem.at[min(t, early)]
        )

    early = min(2, prompts)
    for t in range(prompts):
        x_copy(t).start()

    barrier = pltpu.get_barrier_semaphore()
    xn = tp + 1 - 2 * lax.rem(tp, 2)
    yn = tp + 2 - 4 * (tp // 2)
    far = n_tp - 1 - tp

    @pl.when(sp > 0)
    def _():
        pl.semaphore_signal(barrier, inc=1, device_id={"sp": sp - 1})

    @pl.when(sp < last)
    def _():
        pl.semaphore_signal(barrier, inc=1, device_id={"sp": sp + 1})

    pl.semaphore_signal(barrier, inc=1, device_id={"tp": xn})
    pl.semaphore_signal(barrier, inc=1, device_id={"tp": yn})
    loads = [
        pltpu.make_async_copy(source, target, local_sem.at[k])
        for k, (source, target) in enumerate(
            (
                (gates_hbm, gates_ref),
                (rate_hbm, rate_ref),
                (bias_hbm, bias_ref),
                (extra_hbm, extra_ref),
                (query_hbm, query_ref),
                (gain_hbm, gain_ref),
                (wk_hbm, w.at[:, pl.ds(0, width)]),
                (wv_hbm, w.at[:, pl.ds(width, nh * DV)]),
            )
        )
    ]
    beside = (sp + last - 1) // last + (2 * last - sp - 1) // last
    pl.semaphore_wait(barrier, 2 + beside)

    half = depth // 2

    def part(at):
        return pl.ds(at * half, half)

    def direct(t, way, first):
        p = prompt_at(t)
        block = gath.at[tp, p, :, part(way if first else 1 - way)]
        return pltpu.make_async_remote_copy(
            src_ref=block,
            dst_ref=block,
            send_sem=gsend.at[0],
            recv_sem=grecv.at[way, t] if first else grecv.at[2, t],
            device_id={"tp": xn if way == 0 else yn},
        )

    def passed(t, way):
        block = gath.at[xn if way == 0 else yn, prompt_at(t), :, part(way)]
        return pltpu.make_async_remote_copy(
            src_ref=block,
            dst_ref=block,
            send_sem=gsend.at[0],
            recv_sem=grecv.at[2, t],
            device_id={"tp": yn if way == 0 else xn},
        )

    def start_direct(t, first):
        for way in range(2):
            direct(t, way, first).start()

    def pass_on(t):
        for way in range(2):
            direct(t, way, True).wait_recv()
            passed(t, way).start()

    def gathered(t):
        blocks = gath.at[pl.ds(0, 2), prompt_at(t)]
        pltpu.make_async_remote_copy(
            src_ref=blocks,
            dst_ref=blocks,
            send_sem=gsend.at[0],
            recv_sem=grecv.at[2, t],
            device_id={"tp": xn},
        ).wait_recv()

    def up_copy(t, full):
        return pltpu.make_async_remote_copy(
            src_ref=up_out.at[t] if full else up_out.at[t, 0],
            dst_ref=up_in.at[t] if full else up_in.at[t, 0],
            send_sem=usend.at[lax.rem(t, 2)],
            recv_sem=urecv.at[t],
            device_id={"sp": sp + 1},
        )

    def down_copy(t, full):
        span = pl.ds(0, down_out.shape[1] if full else low_at)
        return pltpu.make_async_remote_copy(
            src_ref=down_out.at[t, span],
            dst_ref=down_in.at[t, span],
            send_sem=dsend.at[lax.rem(t, 2)],
            recv_sem=drecv.at[t],
            device_id={"sp": sp - 1},
        )

    def on_core(which, act):
        pl.when(core == which)(lambda: act(True))
        pl.when(core != which)(lambda: act(False))

    def read_copy(target, source):
        return pltpu.make_async_remote_copy(
            src_ref=read_buf,
            dst_ref=read_land.at[source],
            send_sem=rsend.at[0],
            recv_sem=rrecv.at[0],
            device_id={"sp": target},
        )

    soon = ((tp, 0), (tp, 1), (xn, 0), (yn, 1))
    late = ((far, 0), (far, 1), (xn, 1), (yn, 0))

    def feature(at):
        return pl.ds(pl.multiple_of(at[0] * depth + at[1] * half, half), half)

    def features(p, which):
        return jnp.concatenate([gath[s, p, :, part(k)] for s, k in which], axis=1)

    def gate_rows(which):
        return jnp.concatenate([gsel[:, feature(at)] for at in which], axis=1)

    def weights(which, cols):
        return jnp.concatenate([w[feature(at), cols] for at in which], axis=0)

    levels = 1
    while (1 << levels) < seg:
        levels += 1
    groups = [(k, min(k + 3, levels)) for k in range(1, levels, 3)]
    tile = DK + DV

    def ahead(t):
        p = prompt_at(t)
        slot = lax.rem(t, 2)
        x = features(p, soon)

        def gate_piece():
            gacc[slot] = dot(gate_rows(soon), x, ((1,), (1,)))

        def piece(at):
            def go():
                cols = pl.ds(at * tile, tile)
                acc[slot, :, cols] = dot(x, weights(soon, cols))

            return go

        return [gate_piece] + [piece(at) for at in range(2 * width // tile)]

    def work(t, pieces):
        pieces = list(pieces)

        def fill():
            if pieces:
                pieces.pop(0)()

        p = prompt_at(t)
        slot = lax.rem(t, 2)
        x = features(p, late)
        gt = gacc[slot] + dot(gate_rows(late), x, ((1,), (1,)))
        key_pre = acc[slot, :, :width] + dot(x, weights(late, pl.ds(0, width)))
        gd = gt[:pad]
        gb = gt[pad:]
        extra = jnp.concatenate([extra_ref[p], jnp.zeros((pad - nh, seg), F32)], axis=0)
        soft = jnp.maximum(gd, 0.0) + jnp.log1p(jnp.exp(-jnp.abs(gd)))
        log_decay = extra - fixed[0] * soft
        beta_pre = gb + fixed[1]
        beta = jax.nn.sigmoid(beta_pre)
        log_beta = jnp.minimum(beta_pre, 0.0) - jnp.log1p(jnp.exp(-jnp.abs(beta_pre)))
        high = log_decay.astype(BF).astype(F32)
        rest = log_decay - high
        mid = rest.astype(BF).astype(F32)
        split = jnp.concatenate([high, mid, rest - mid, jnp.zeros_like(high)], axis=0)
        sums = dot(split.astype(BF), upper[...])
        run = sums[:pad] + sums[pad : 2 * pad] + sums[2 * pad : 3 * pad]
        end = run[:, seg - 1 : seg]
        decs[p] = jnp.broadcast_to(jnp.exp(end), (pad, DV))
        cols = jnp.concatenate(
            [run + log_beta, beta, beta * jnp.exp(run), jnp.exp(end - run)], axis=0
        ).T
        lev = level[...]
        strict = lev >= 0
        eye = jnp.where(
            lax.broadcasted_iota(jnp.int32, (seg, seg), 0)
            == lax.broadcasted_iota(jnp.int32, (seg, seg), 1),
            1.0,
            0.0,
        ).astype(F32)
        hs = range(nh)
        keys, grams = [], []
        for h in hs:
            pre = key_pre[:, h * DK : (h + 1) * DK]
            raw = pre * jax.nn.sigmoid(pre)
            key = raw * lax.rsqrt(jnp.sum(raw * raw, axis=-1, keepdims=True) + EPS)
            kb = key.astype(BF)
            keys.append(key)
            grams.append(dot(kb, kb, ((1,), (1,))))
        value_pre = acc[slot, :, width:] + dot(x, weights(late, pl.ds(width, nh * DV)))
        fill()
        fill()
        lower, inv = [], []
        for h in hs:
            spread = cols[:, h : h + 1] - run[h : h + 1, :]
            low = jnp.where(strict, grams[h] * jnp.exp(jnp.where(strict, spread, 0.0)), 0.0)
            lower.append(low)
            inv.append(eye - jnp.where(lev == 0, low, 0.0))

        def merge(first, until):
            inside = jnp.logical_and(lev >= first, lev < until)
            cuts = [jnp.where(inside, low, 0.0).astype(BF) for low in lower]
            return [dot(f.astype(BF), cut).astype(BF) for f, cut in zip(inv, cuts)]

        for first, until in groups[:-1]:
            steps = merge(first, until)
            fill()
            for k in range(first, until - 1):
                both = [
                    dot(e, jnp.concatenate([e, f.astype(BF)], axis=1))
                    for e, f in zip(steps, inv)
                ]
                steps = [b[:, :seg].astype(BF) for b in both]
                fill()
                inv = [f - b[:, seg:] if k == first else f + b[:, seg:] for f, b in zip(inv, both)]
            one = until - 1 == first
            moves = [dot(e, f.astype(BF)) for e, f in zip(steps, inv)]
            inv = [f - m if one else f + m for f, m in zip(inv, moves)]
        sides = []
        for h in hs:
            pre = value_pre[:, h * DV : (h + 1) * DV]
            value = pre * jax.nn.sigmoid(pre)
            sides.append(
                jnp.concatenate(
                    [
                        value * cols[:, pad + h : pad + h + 1],
                        keys[h] * cols[:, 2 * pad + h : 2 * pad + h + 1],
                    ],
                    axis=1,
                )
            )
        first, until = groups[-1]
        steps = merge(first, until)
        sides = [
            side + dot((f - eye).astype(BF), side.astype(BF)) for f, side in zip(inv, sides)
        ]
        fill()
        sides = [side - dot(e, side.astype(BF)) for e, side in zip(steps, sides)]
        for _ in range(first + 1, until):
            steps = [dot(e, e).astype(BF) for e in steps]
            fill()
            sides = [side + dot(e, side.astype(BF)) for e, side in zip(steps, sides)]
        while pieces:
            fill()
        tall = ((0,), (0,))
        for h in hs:
            faded = keys[h] * cols[:, 3 * pad + h : 3 * pad + h + 1]
            late_top = faded.astype(BF)
            late_rest = (faded - late_top.astype(F32)).astype(BF)
            top = sides[h].astype(BF)
            rest = (sides[h][:, :DV] - top[:, :DV].astype(F32)).astype(BF)
            both = dot(
                jnp.concatenate([late_top, late_rest], axis=0),
                jnp.concatenate([top, top], axis=0),
                tall,
            )
            adds[p, h] = both[:, :DV] + dot(late_top, rest, tall)
            maps[p, h] = both[:, DV:].astype(BF)

    def moved(at, p, h):
        top = up_in[at, 0, h]
        state = top.astype(F32) + up_in[at, 1, h].astype(F32)
        return decs[p, pl.ds(h, 1)] * state + adds[p, h] - dot(maps[p, h], top)

    def go_up(t, p, fresh):
        for h in range(nh):
            state = adds[p, h] if fresh else moved(t - 1, p, h)
            top = state.astype(BF)
            up_out[t, 0, h] = top
            up_out[t, 1, h] = (state - top.astype(F32)).astype(BF)

    def later(at):
        terms = down_in[at, pl.ds(0, map_at)].astype(F32)
        return terms[:pad] + terms[pad : 2 * pad] + terms[2 * pad : 3 * pad]

    def rows(first, h):
        return pl.ds(first + h * DK, DK)

    def total(at, h):
        top = down_in[at, rows(add_at, h)].astype(F32)
        return top + down_in[at, rows(low_at, h)].astype(F32)

    def go_down(t, p, fresh):
        own = decs[p]
        dec = None if fresh else later(t - 1)
        for h in range(nh):
            add = adds[p, h]
            if fresh:
                down_out[t, rows(map_at, h)] = maps[p, h]
            else:
                above = down_in[t - 1, rows(map_at, h)]
                own_map = maps[p, h]
                turn = dot(above, jnp.concatenate([own_map, add.astype(BF)], axis=1))
                add = dec[h : h + 1] * add + total(t - 1, h) - turn[:, DK:]
                both = dec[h : h + 1] * own_map.astype(F32) + own[h : h + 1] * above.astype(F32)
                down_out[t, rows(map_at, h)] = (both - turn[:, :DK]).astype(BF)
            top = add.astype(BF)
            down_out[t, rows(add_at, h)] = top
            down_out[t, rows(low_at, h)] = (add - top.astype(F32)).astype(BF)
        dec = own if fresh else own * dec
        high = dec.astype(BF).astype(F32)
        rest = dec - high
        mid = rest.astype(BF).astype(F32)
        split = jnp.concatenate([high, mid, rest - mid, jnp.zeros_like(high)], axis=0)
        down_out[t, pl.ds(0, map_at)] = split.astype(BF)

    def wait_up(t):
        on_core(1, lambda full: up_copy(t, full).wait_recv())

    def wait_down(t):
        on_core(0, lambda full: down_copy(t, full).wait_recv())

    def chain_up(t):
        rev = last - t

        @pl.when(sp + rev <= last)
        def _():
            @pl.when(sp == 0)
            def _():
                go_up(t, rev, True)

            @pl.when(sp > 0)
            def _():
                wait_up(t - 1)
                go_up(t, sp + rev, False)

            @pl.when(sp + rev + 2 <= last)
            def _():
                on_core(0, lambda full: up_copy(t - 2, full).wait_send())

            on_core(0, lambda full: up_copy(t, full).start())

    def chain_down(t):
        rev = last - t

        @pl.when(sp >= rev)
        def _():
            @pl.when(sp == last)
            def _():
                go_down(t, last - rev, True)

            @pl.when(sp < last)
            def _():
                wait_down(t - 1)
                go_down(t, sp - rev, False)

            @pl.when(sp >= rev + 2)
            def _():
                on_core(1, lambda full: down_copy(t - 2, full).wait_send())

            on_core(1, lambda full: down_copy(t, full).start())

    def before(t):
        pl.when(core == 0)(lambda: chain_down(t))
        pl.when(core == 1)(lambda: chain_up(t))

    def after(t):
        pl.when(core == 0)(lambda: chain_up(t))
        pl.when(core == 1)(lambda: chain_down(t))

    def close(below, above):
        at = last - 1
        dec = later(at) if above else None
        for h in range(nh):
            state = moved(at, sp, h) if below else adds[sp, h]
            if above:
                state = (
                    dec[h : h + 1] * state
                    + total(at, h)
                    - dot(down_in[at, rows(map_at, h)], state.astype(BF))
                )
            cached = state.astype(BF)
            state_out[:, h * DV : (h + 1) * DV] = cached
            raw = dot(query[h].astype(BF), cached)
            norm = (
                raw
                * lax.rsqrt(jnp.mean(raw * raw, axis=-1, keepdims=True) + EPS)
                * gain_ref[...]
            )
            read_buf[pl.ds(h, 1)] = norm[:1]

    for t in range(early):
        x_copy(t).wait()
        start_direct(t, True)
        if t == 0:
            start_direct(t, False)
    for load in loads:
        load.start()
    if early < prompts:
        others = pl.ds(0, prompts - early)
        pltpu.make_async_copy(
            x_hbm.at[others], gath.at[tp, others], x_sem.at[early]
        ).wait()
    for load in loads[:6]:
        load.wait()

    r_id = lax.broadcasted_iota(jnp.int32, (seg, seg), 0)
    c_id = lax.broadcasted_iota(jnp.int32, (seg, seg), 1)
    lev = jnp.zeros((seg, seg), jnp.int32)
    k = 1
    while (1 << k) < seg:
        lev = jnp.where((r_id >> k) != (c_id >> k), k, lev)
        k += 1
    level[...] = jnp.where(r_id > c_id, lev, -1)
    upper[...] = jnp.where(r_id <= c_id, 1.0, 0.0).astype(BF)

    row_id = lax.broadcasted_iota(jnp.int32, (pad, seg), 0)
    rate = jnp.zeros((pad, seg), F32)
    bias = jnp.zeros((pad, seg), F32)
    for h in range(nh):
        rate = jnp.where(row_id == h, rate_ref[h], rate)
        bias = jnp.where(row_id == h, bias_ref[h], bias)
    fixed[0] = rate
    fixed[1] = bias
    for at in range(n_tp * depth // 128):
        chunk = gates_ref[:, at * 128 : (at + 1) * 128].astype(F32)
        gall[at, pl.ds(0, heads)] = chunk[:heads]
        gall[at, pl.ds(heads, heads)] = chunk[heads:]
        gall[at, pl.ds(2 * heads, pad)] = jnp.zeros((pad, 128), F32)
        picked = [gall[at, pl.ds(tp * nh + k * heads, pad)] for k in range(2)]
        gsel[:, at * 128 : (at + 1) * 128] = jnp.concatenate(picked, axis=0).astype(BF)
    every = query_ref[...].astype(F32)
    mine = lax.broadcasted_iota(jnp.int32, every.shape, 0) == sp
    asked = jnp.sum(jnp.where(mine, every, 0.0), axis=0, keepdims=True)
    for h in range(nh):
        query[h] = jnp.broadcast_to(asked[:, h * DK : (h + 1) * DK], (pad, DK))
    read_buf[...] = jnp.zeros_like(read_buf)

    @pl.when(core == 0)
    def _():
        up_in[:, 1] = jnp.zeros((n_sp - 1, nh, DK, DV), BF)

    @pl.when(core == 1)
    def _():
        down_in[:, pl.ds(low_at, nh * DK)] = jnp.zeros((n_sp - 1, nh * DK, DV), BF)


    pass_on(0)
    start_direct(1, False)
    if early < prompts:
        start_direct(early, True)
    for load in loads[6:]:
        load.wait()
    for go in ahead(0):
        go()

    def body(t, carry):
        pass_on(t + 1)

        @pl.when(t + 2 < prompts)
        def _():
            start_direct(t + 2, False)

        @pl.when(t + 3 < prompts)
        def _():
            start_direct(t + 3, True)

        gathered(t)
        before(t)
        work(t, ahead(t + 1))
        after(t)
        return carry

    lax.fori_loop(0, last, body, 0)
    gathered(last)
    work(last, [])

    @pl.when(sp > 0)
    def _():
        wait_up(last - 1)

    @pl.when(sp < last)
    def _():
        wait_down(last - 1)

    @pl.when(sp == 0)
    def _():
        close(False, True)

    @pl.when(jnp.logical_and(sp > 0, sp < last))
    def _():
        close(True, True)

    @pl.when(sp == last)
    def _():
        close(True, False)

    def tell(step, carry):
        target = lax.rem(sp + step, n_sp)
        read_copy(target, sp).start()
        return carry

    lax.fori_loop(1, n_sp, tell, 0)
    read_land[sp] = read_buf[...]

    block = gath.at[pl.ds(0, n_tp - 1)]
    pltpu.make_async_remote_copy(
        src_ref=block,
        dst_ref=block,
        send_sem=gsend.at[0],
        recv_sem=grecv.at[2, 0],
        device_id={"tp": xn},
    ).wait_send()

    for back in range(1, min(last, 2) + 1):

        @pl.when(sp + back <= last)
        def _():
            on_core(0, lambda full: up_copy(last - back, full).wait_send())

        @pl.when(sp >= back)
        def _():
            on_core(1, lambda full: down_copy(last - back, full).wait_send())

    others = read_land.at[pl.ds(0, last)]
    reads = pltpu.make_async_remote_copy(
        src_ref=others,
        dst_ref=others,
        send_sem=rsend.at[0],
        recv_sem=rrecv.at[0],
        device_id={"sp": lax.rem(sp + 1, n_sp)},
    )
    reads.wait_send()
    reads.wait_recv()
    for h in range(nh):
        read_out[:, h * DV : (h + 1) * DV] = read_land[:, h].astype(BF)


def hand_over(state, read, state_out, read_out, sems):
    pairs = ((state, state_out), (read, read_out))
    copies = [pltpu.make_async_copy(a, b, sems.at[k]) for k, (a, b) in enumerate(pairs)]
    for copy in copies:
        copy.start()
    for copy in copies:
        copy.wait()


def close_by(n_sp, n_tp, prompts, seg, depth, rows, nh):
    paired = n_sp >= 4 and n_sp & (n_sp - 1) == 0 and n_tp == 4
    whole = prompts == n_sp and rows == DK and 1 <= nh <= 8
    return paired and whole and seg == 128 and depth % 256 == 0


def shards(
    n_sp,
    n_tp,
    layer_input,
    w_key,
    w_value,
    w_gates,
    decay_rate,
    beta_bias,
    log_decay_extra,
    new_query,
    read_gain,
):
    prompts, seg, depth = layer_input.shape
    whole_depth, width = w_key.shape
    nh = width // DK
    heads = w_gates.shape[2]
    rows = prompts * DK // n_sp
    share = max(nh // 2, 1)
    gates = jnp.swapaxes(w_gates, 1, 2).reshape(2 * heads, whole_depth)
    vmem = pl.BlockSpec(memory_space=pltpu.VMEM)
    smem = pl.BlockSpec(memory_space=pltpu.SMEM)
    hbm = pl.BlockSpec(memory_space=pl.ANY)
    dma = pltpu.SemaphoreType.DMA
    if close_by(n_sp, n_tp, prompts, seg, depth, rows, nh):
        hops = n_sp - 1
        made = pl.pallas_call(
            functools.partial(near, n_sp, n_tp, nh),
            out_shape=(
                pltpu.VMEM((rows, nh * DV), BF),
                pltpu.VMEM((prompts, nh * DV), BF),
            ),
            in_specs=[hbm] * 9,
            out_specs=(vmem, vmem),
            scratch_shapes=[
                pltpu.VMEM((2 * heads, whole_depth), BF),
                pltpu.SMEM((nh,), F32),
                pltpu.SMEM((nh,), F32),
                pltpu.VMEM((prompts, nh, seg), F32),
                pltpu.VMEM((prompts, nh * DK), BF),
                pltpu.VMEM((1, DV), F32),
                pltpu.VMEM((n_tp, prompts, seg, depth), BF),
                pltpu.VMEM((whole_depth, nh * (DK + DV)), BF),
                pltpu.VMEM((whole_depth // 128, 2 * heads + 8, 128), F32),
                pltpu.VMEM((16, whole_depth), BF),
                pltpu.VMEM((2, 8, seg), F32),
                pltpu.VMEM((seg, seg), jnp.int32),
                pltpu.VMEM((seg, seg), BF),
                pltpu.VMEM((2, seg, nh * (DK + DV)), F32),
                pltpu.VMEM((2, 16, seg), F32),
                pltpu.VMEM((prompts, nh, DK, DK), BF),
                pltpu.VMEM((prompts, nh, DK, DV), F32),
                pltpu.VMEM((prompts, 8, DV), F32),
                pltpu.VMEM((hops, 2, nh, DK, DV), BF),
                pltpu.VMEM((hops, 2, nh, DK, DV), BF),
                pltpu.VMEM((hops, 32 + 3 * nh * DK, DV), BF),
                pltpu.VMEM((hops, 32 + 3 * nh * DK, DV), BF),
                pltpu.VMEM((nh, 8, DK), F32),
                pltpu.VMEM((8, DV), F32),
                pltpu.VMEM((prompts, 8, DV), F32),
                dma((8,)),
                dma((min(2, prompts) + 1,)),
                dma((1,)),
                dma((3, prompts)),
                dma((2,)),
                dma((hops,)),
                dma((2,)),
                dma((hops,)),
                dma((1,)),
                dma((1,)),
            ],
            compiler_params=pltpu.CompilerParams(
                collective_id=0, has_side_effects=True, vmem_limit_bytes=56 * 1024 * 1024
            ),
        )(
            layer_input,
            w_key,
            w_value,
            gates,
            decay_rate,
            beta_bias,
            log_decay_extra,
            new_query,
            read_gain.reshape(1, DV),
        )
        return pl.pallas_call(
            hand_over,
            out_shape=tuple(jax.ShapeDtypeStruct(a.shape, a.dtype) for a in made),
            in_specs=[vmem, vmem],
            out_specs=(hbm, hbm),
            scratch_shapes=[dma((2,))],
        )(*[pltpu.with_memory_space_constraint(a, pltpu.VMEM) for a in made])
    return pl.pallas_call(
        functools.partial(kernel, n_sp, n_tp, nh, rows),
        out_shape=(
            jax.ShapeDtypeStruct((rows, nh * DV), BF),
            jax.ShapeDtypeStruct((prompts, nh * DV), BF),
        ),
        in_specs=[hbm, hbm, hbm, vmem, smem, smem, vmem, vmem, vmem],
        out_specs=(vmem, vmem),
        scratch_shapes=[
            pltpu.VMEM((n_tp, prompts, seg, depth), BF),
            pltpu.VMEM((whole_depth, nh * (DK + DV)), BF),
            pltpu.VMEM((2, heads + 8, seg), F32),
            pltpu.VMEM((seg, seg), jnp.int32),
            pltpu.VMEM((seg, seg), F32),
            pltpu.VMEM((prompts, nh, DK, DK), BF),
            pltpu.VMEM((prompts, nh, DK, DV), F32),
            pltpu.VMEM((prompts, 8, DV), F32),
            pltpu.VMEM((prompts, share, DK, DK), BF),
            pltpu.VMEM((prompts, share, DK, DV), F32),
            pltpu.VMEM((prompts, 8, DV), F32),
            pltpu.VMEM((prompts, 8, DV), F32),
            pltpu.VMEM((prompts, share, DK, DV), BF),
            pltpu.VMEM((prompts, share, DK, DV), BF),
            pltpu.VMEM((prompts, share, DK, DV), BF),
            pltpu.VMEM((nh, rows, DV), BF),
            pltpu.VMEM((share, prompts, DV), F32),
            pltpu.VMEM((nh, prompts, DV), F32),
            pltpu.VMEM((nh, prompts, DK), BF),
            dma((3,)),
            dma((max(n_tp, 4), prompts)),
            dma((max(n_tp, 4), prompts)),
            dma((3, prompts)),
            dma((3, prompts)),
            dma((prompts, share)),
            dma((prompts, share)),
            dma((prompts, DK // rows)),
            dma((2,)),
            dma((n_sp,)),
            dma((2,)),
        ],
        compiler_params=pltpu.CompilerParams(
            collective_id=0, has_side_effects=True, vmem_limit_bytes=56 * 1024 * 1024
        ),
    )(
        layer_input,
        w_key,
        w_value,
        gates,
        decay_rate,
        beta_bias,
        log_decay_extra,
        new_query,
        read_gain.reshape(1, DV),
    )


def solution(mesh):
    return jax.shard_map(
        functools.partial(shards, mesh.shape["sp"], mesh.shape["tp"]),
        mesh=mesh,
        in_specs=(
            P(None, "sp", "tp"),
            P(None, "tp"),
            P(None, "tp"),
            P(),
            P("tp"),
            P("tp"),
            P(None, "tp", "sp"),
            P(None, "tp"),
            P(),
        ),
        out_specs=(P("sp", "tp"), P(None, "tp")),
        check_vma=False,
    )
```

```python
import functools

import jax
import jax.numpy as jnp
from jax import lax
from jax.experimental import pallas as pl
from jax.experimental.pallas import tpu as pltpu
from jax.sharding import PartitionSpec as P

DK = 128
DV = 128
EPS = 1e-06
HIGH = lax.Precision.HIGHEST
BF = jnp.bfloat16
F32 = jnp.float32


def dot(left, right, dims=((1,), (0,)), precision=None):
    return lax.dot_general(
        left, right, (dims, ((), ())), precision=precision, preferred_element_type=F32
    )


def kernel(
    n_sp,
    n_tp,
    nh,
    rows,
    x_hbm,
    wk_hbm,
    wv_hbm,
    gates_ref,
    rate_ref,
    bias_ref,
    extra_ref,
    query_ref,
    gain_ref,
    state_out,
    read_out,
    gath,
    w,
    graw,
    level,
    upper,
    maps,
    adds,
    decs,
    pair_maps,
    pair_adds,
    pair_decs,
    joint_decs,
    came,
    sent,
    final,
    landing,
    read_buf,
    read_land,
    query_heads,
    local_sem,
    gsend,
    grecv,
    psend,
    precv,
    csend,
    crecv,
    ssend,
    srecv,
    rsend,
    rrecv,
):
    prompts, seg, depth = x_hbm.shape
    width = nh * DK
    heads = gates_ref.shape[0] // 2
    sp = lax.axis_index("sp")
    tp = lax.axis_index("tp")
    core = lax.rem(sp, 2)
    other = 1 - core
    chip = sp // 2
    last_chip = n_sp // 2 - 1
    share = max(nh // 2, 1)
    mine = core * share
    theirs = other * share
    has_mine = mine < nh
    has_theirs = theirs < nh
    sources = [k for k in range(2) if k * share < nh]
    chunks = DK // rows
    relay = n_tp == 4

    x_copy = pltpu.make_async_copy(x_hbm, gath.at[tp], local_sem.at[0])
    x_copy.start()
    wk_copy = pltpu.make_async_copy(wk_hbm, w.at[:, pl.ds(0, width)], local_sem.at[1])
    wv_copy = pltpu.make_async_copy(wv_hbm, w.at[:, pl.ds(width, nh * DV)], local_sem.at[2])
    wk_copy.start()
    wv_copy.start()

    barrier = pltpu.get_barrier_semaphore()

    def greet_tp(step, carry):
        pl.semaphore_signal(barrier, inc=1, device_id={"tp": lax.rem(tp + step, n_tp)})
        return carry

    def greet_sp(step, carry):
        pl.semaphore_signal(barrier, inc=1, device_id={"sp": lax.rem(sp + step, n_sp)})
        return carry

    lax.fori_loop(1, n_tp, greet_tp, 0)
    lax.fori_loop(1, n_sp, greet_sp, 0)
    r_id = lax.broadcasted_iota(jnp.int32, (seg, seg), 0)
    c_id = lax.broadcasted_iota(jnp.int32, (seg, seg), 1)
    lev = jnp.zeros((seg, seg), jnp.int32)
    k = 1
    while (1 << k) < seg:
        lev = jnp.where((r_id >> k) != (c_id >> k), k, lev)
        k += 1
    levels = k
    level[...] = jnp.where(r_id > c_id, lev, -1)
    upper[...] = jnp.where(r_id <= c_id, 1.0, 0.0).astype(F32)
    graw[...] = jnp.zeros_like(graw)
    pl.semaphore_wait(barrier, n_tp - 1 + n_sp - 1)
    x_copy.wait()

    xn = tp + 1 - 2 * lax.rem(tp, 2)
    yn = tp + 2 - 4 * (tp // 2)
    half = seg // 2

    def direct(p, way):
        target = xn if way == 0 else yn
        return pltpu.make_async_remote_copy(
            src_ref=gath.at[tp, p],
            dst_ref=gath.at[tp, p],
            send_sem=gsend.at[way, p],
            recv_sem=grecv.at[way, p],
            device_id={"tp": target},
        )

    def passed(p, way):
        source = xn if way == 0 else yn
        target = yn if way == 0 else xn
        part = pl.ds(way * half, half)
        return pltpu.make_async_remote_copy(
            src_ref=gath.at[source, p, part],
            dst_ref=gath.at[source, p, part],
            send_sem=gsend.at[2 + way, p],
            recv_sem=grecv.at[2 + way, p],
            device_id={"tp": target},
        )

    def plain(p, step):
        return pltpu.make_async_remote_copy(
            src_ref=gath.at[tp, p],
            dst_ref=gath.at[tp, p],
            send_sem=gsend.at[step, p],
            recv_sem=grecv.at[step, p],
            device_id={"tp": lax.rem(tp + step, n_tp)},
        )

    def start_direct(p):
        direct(p, 0).start()
        direct(p, 1).start()

    def pass_on(p):
        direct(p, 0).wait_recv()
        passed(p, 0).start()
        direct(p, 1).wait_recv()
        passed(p, 1).start()

    early = min(2, prompts)
    ahead = min(1, prompts)
    if relay:
        for p in range(early):
            start_direct(p)
        for p in range(ahead):
            pass_on(p)
            if early + p < prompts:
                start_direct(early + p)
    else:

        def start_plain(index, carry):
            plain(index // (n_tp - 1), lax.rem(index, n_tp - 1) + 1).start()
            return carry

        lax.fori_loop(0, prompts * (n_tp - 1), start_plain, 0)
    wk_copy.wait()
    wv_copy.wait()

    def pair_copies(p):
        pairs = (
            (maps.at[p, pl.ds(theirs, share)], pair_maps.at[p]),
            (adds.at[p, pl.ds(theirs, share)], pair_adds.at[p]),
            (decs.at[p], pair_decs.at[p]),
        )
        return [
            pltpu.make_async_remote_copy(
                src_ref=source,
                dst_ref=target,
                send_sem=psend.at[i, p],
                recv_sem=precv.at[i, p],
                device_id={"sp": sp + 1 - 2 * core},
            )
            for i, (source, target) in enumerate(pairs)
        ]

    def chain_copy(p, j):
        return pltpu.make_async_remote_copy(
            src_ref=sent.at[p, j],
            dst_ref=came.at[p, j],
            send_sem=csend.at[p, j],
            recv_sem=crecv.at[p, j],
            device_id={"sp": lax.rem(sp + 2, n_sp)},
        )

    def state_copy(p, c, slot):
        return pltpu.make_async_remote_copy(
            src_ref=final.at[p, :, pl.ds(c * rows, rows)],
            dst_ref=landing.at[pl.ds(slot * share, share)],
            send_sem=ssend.at[p, c],
            recv_sem=srecv.at[slot],
            device_id={"sp": p * chunks + c},
        )

    def read_copy(target, slot):
        return pltpu.make_async_remote_copy(
            src_ref=read_buf,
            dst_ref=read_land.at[pl.ds(slot * share, share)],
            send_sem=rsend.at[target],
            recv_sem=rrecv.at[slot],
            device_id={"sp": target},
        )

    first_head = tp * nh
    pad = 8
    row_id = lax.broadcasted_iota(jnp.int32, (pad, seg), 0)

    def work(p):
        x = jnp.concatenate([gath[s, p] for s in range(n_tp)], axis=1)
        pre = dot(x, w[...])
        gt = dot(gates_ref[...], x, ((1,), (1,)))
        graw[0, pl.ds(0, heads)] = gt[:heads]
        graw[1, pl.ds(0, heads)] = gt[heads:]
        gd = graw[0, pl.ds(first_head, pad)]
        gb = graw[1, pl.ds(first_head, pad)]
        rate = jnp.zeros((pad, seg), F32)
        bias = jnp.zeros((pad, seg), F32)
        for h in range(nh):
            rate = jnp.where(row_id == h, rate_ref[h], rate)
            bias = jnp.where(row_id == h, bias_ref[h], bias)
        extra = jnp.concatenate([extra_ref[p], jnp.zeros((pad - nh, seg), F32)], axis=0)
        soft = jnp.maximum(gd, 0.0) + jnp.log1p(jnp.exp(-jnp.abs(gd)))
        log_decay = extra - rate * soft
        beta = jax.nn.sigmoid(gb + bias)
        run = dot(log_decay, upper[...], precision=HIGH)
        end = run[:, seg - 1 : seg]
        decs[p] = jnp.broadcast_to(jnp.exp(end), (pad, DV))
        cols = jnp.concatenate(
            [run, beta, beta * jnp.exp(run), jnp.exp(end - run)], axis=0
        ).T
        act = pre * jax.nn.sigmoid(pre)
        lev = level[...]
        strict = lev >= 0
        eye = jnp.where(
            lax.broadcasted_iota(jnp.int32, (seg, seg), 0)
            == lax.broadcasted_iota(jnp.int32, (seg, seg), 1),
            1.0,
            0.0,
        ).astype(F32)
        keys, lower, inv = [], [], []
        for h in range(nh):
            raw = act[:, h * DK : (h + 1) * DK]
            key = raw * lax.rsqrt(jnp.sum(raw * raw, axis=-1, keepdims=True) + EPS)
            kb = key.astype(BF)
            gram = dot(kb, kb, ((1,), (1,)))
            spread = cols[:, h : h + 1] - run[h : h + 1, :]
            weight = jnp.exp(jnp.where(strict, spread, 0.0))
            low = jnp.where(strict, gram * weight * cols[:, pad + h : pad + h + 1], 0.0)
            keys.append(key)
            lower.append(low)
            inv.append(jnp.where(lev == 0, -low, 0.0))
        for step in range(1, levels):
            cuts = [jnp.where(lev == step, low, 0.0) for low in lower]
            full = [(eye + part).astype(BF) for part in inv]
            mids = [dot(cut.astype(BF), f) for cut, f in zip(cuts, full)]
            inv = [
                part - dot(f, mid.astype(BF)) for part, f, mid in zip(inv, full, mids)
            ]
        for h in range(nh):
            value = act[:, width + h * DV : width + (h + 1) * DV]
            side = jnp.concatenate(
                [
                    value * cols[:, pad + h : pad + h + 1],
                    keys[h] * cols[:, 2 * pad + h : 2 * pad + h + 1],
                ],
                axis=1,
            )
            solved = side + dot(inv[h].astype(BF), side.astype(BF))
            late = keys[h] * cols[:, 3 * pad + h : 3 * pad + h + 1]
            late_top = late.astype(BF)
            late_rest = (late - late_top.astype(F32)).astype(BF)
            top = solved.astype(BF)
            rest = (solved[:, :DV] - top[:, :DV].astype(F32)).astype(BF)
            tall = ((0,), (0,))
            both = dot(late_top, top, tall)
            adds[p, h] = (
                both[:, :DV] + dot(late_top, rest, tall) + dot(late_rest, top[:, :DV], tall)
            )
            maps[p, h] = both[:, DV:].astype(BF)

    def unite(p):
        def merge(j, early, late, early_dec, late_dec):
            h = mine + j
            map_0, add_0 = early[0][...], early[1][...]
            map_1, add_1 = late[0][...], late[1][...]
            dec_0 = early_dec[p, pl.ds(h, 1)]
            dec_1 = late_dec[p, pl.ds(h, 1)]
            turn = dot(map_1, jnp.concatenate([map_0, add_0.astype(BF)], axis=1))
            maps[p, h] = (
                dec_1 * map_0.astype(F32) + dec_0 * map_1.astype(F32) - turn[:, :DK]
            ).astype(BF)
            adds[p, h] = dec_1 * add_0 + add_1 - turn[:, DK:]

        @pl.when(has_mine)
        def _():
            for copy in pair_copies(p):
                copy.wait_recv()
            joint_decs[p] = decs[p] * pair_decs[p]
            for first in range(2):

                @pl.when(core == first)
                def _():
                    for j in range(share):
                        own = (maps.at[p, mine + j], adds.at[p, mine + j])
                        got = (pair_maps.at[p, j], pair_adds.at[p, j])
                        if first == 0:
                            merge(j, own, got, decs, pair_decs)
                        else:
                            merge(j, got, own, pair_decs, decs)

    def advance(p):
        @pl.when(chip == 0)
        def _():
            for j in range(share):
                sent[p, j] = adds[p, mine + j].astype(BF)
                chain_copy(p, j).start()

        def moved(j):
            chain_copy(p, j).wait_recv()
            state = came[p, j]
            h = mine + j
            return (
                joint_decs[p, pl.ds(h, 1)] * state.astype(F32)
                + adds[p, h]
                - dot(maps[p, h], state)
            )

        @pl.when(jnp.logical_and(chip > 0, chip < last_chip))
        def _():
            for j in range(share):
                sent[p, j] = moved(j).astype(BF)
                chain_copy(p, j).start()

        @pl.when(chip == last_chip)
        def _():
            for j in range(share):
                state = moved(j).astype(BF)
                final[p, j] = state
                raw = dot(query_heads[mine + j], state)
                norm = (
                    raw
                    * lax.rsqrt(jnp.mean(raw * raw, axis=-1, keepdims=True) + EPS)
                    * gain_ref[...]
                )
                at_p = lax.broadcasted_iota(jnp.int32, norm.shape, 0) == p
                read_buf[j] = jnp.where(at_p, norm, read_buf[j])
            for c in range(chunks):
                owner = p * chunks + c

                @pl.when(owner != sp)
                def _():
                    state_copy(p, c, core).start()

                @pl.when(owner == sp)
                def _():
                    for j in range(share):
                        landing[mine + j] = final[p, j, c * rows : (c + 1) * rows]

    ending = jnp.logical_and(chip == last_chip, has_mine)

    @pl.when(ending)
    def _():
        read_buf[...] = jnp.zeros_like(read_buf)
        for h in range(nh):
            query_heads[h] = query_ref[:, h * DK : (h + 1) * DK]

    lag = 1 + chip

    def body(it, carry):
        if relay:

            @pl.when(it + ahead < prompts)
            def _():
                pass_on(it + ahead)

            @pl.when(it + ahead + early < prompts)
            def _():
                start_direct(it + ahead + early)

        @pl.when(it < prompts)
        def _():
            if relay:
                passed(it, 0).wait_recv()
                passed(it, 1).wait_recv()
            else:

                def take(step, carry):
                    plain(it, step).wait_recv()
                    return carry

                lax.fori_loop(1, n_tp, take, 0)
            work(it)

            @pl.when(has_theirs)
            def _():
                for copy in pair_copies(it):
                    copy.start()

        @pl.when(jnp.logical_and(it >= 1, it < prompts + 1))
        def _():
            unite(it - 1)

        moving = jnp.logical_and(it >= lag, it < prompts + lag)

        @pl.when(jnp.logical_and(moving, has_mine))
        def _():
            advance(it - lag)

        return carry

    lax.fori_loop(0, prompts + last_chip + 1, body, 0)

    @pl.when(ending)
    def _():
        def tell(target, carry):
            @pl.when(target != sp)
            def _():
                read_copy(target, core).start()

            return carry

        lax.fori_loop(0, n_sp, tell, 0)
        for j in range(share):
            read_land[mine + j] = read_buf[j]

    for k in sources:

        @pl.when(sp != 2 * last_chip + k)
        def _():
            state_copy(0, 0, k).wait_recv()
            read_copy(0, k).wait_recv()

    for h in range(nh):
        state_out[:, h * DV : (h + 1) * DV] = landing[h]
        read_out[:, h * DV : (h + 1) * DV] = read_land[h].astype(BF)

    @pl.when(ending)
    def _():
        def told(target, carry):
            @pl.when(target != sp)
            def _():
                read_copy(target, core).wait_send()
                state_copy(target // chunks, lax.rem(target, chunks), core).wait_send()

            return carry

        lax.fori_loop(0, n_sp, told, 0)

    @pl.when(jnp.logical_and(chip < last_chip, has_mine))
    def _():
        def left(index, carry):
            chain_copy(index // share, lax.rem(index, share)).wait_send()
            return carry

        lax.fori_loop(0, prompts * share, left, 0)

    @pl.when(has_theirs)
    def _():
        def lent(index, carry):
            for copy in pair_copies(index):
                copy.wait_send()
            return carry

        lax.fori_loop(0, prompts, lent, 0)

    def freed(index, carry):
        if relay:
            direct(index, 0).wait_send()
            direct(index, 1).wait_send()
            passed(index, 0).wait_send()
            passed(index, 1).wait_send()
        else:
            for step in range(1, n_tp):
                plain(index, step).wait_send()
        return carry

    lax.fori_loop(0, prompts, freed, 0)


def near(
    n_sp,
    n_tp,
    nh,
    x_hbm,
    wk_hbm,
    wv_hbm,
    gates_hbm,
    rate_hbm,
    bias_hbm,
    extra_hbm,
    query_hbm,
    gain_hbm,
    state_out,
    read_out,
    gates_ref,
    rate_ref,
    bias_ref,
    extra_ref,
    query_ref,
    gain_ref,
    gath,
    w,
    gall,
    gsel,
    fixed,
    level,
    upper,
    acc,
    gacc,
    maps,
    adds,
    decs,
    up_out,
    up_in,
    down_out,
    down_in,
    query,
    read_buf,
    read_land,
    local_sem,
    x_sem,
    gsend,
    grecv,
    usend,
    urecv,
    dsend,
    drecv,
    rsend,
    rrecv,
):
    prompts, seg, depth = x_hbm.shape
    width = nh * DK
    heads = gates_ref.shape[0] // 2
    pad = 8
    last = n_sp - 1
    sp = lax.axis_index("sp")
    tp = lax.axis_index("tp")
    core = lax.rem(sp, 2)
    chip = sp // 2
    chips = n_sp // 2
    map_at = 4 * pad
    add_at = map_at + nh * DK
    low_at = add_at + nh * DK

    def prompt_at(t):
        rev = chips - 1 - t // 2
        owner = 0
        k = 1
        while k < chips:
            owner = owner + k * lax.rem(chip // k + rev // k, 2)
            k *= 2
        flip = (2 * (owner - chip) + 1 - core + n_sp - 1) // n_sp
        return 2 * owner + lax.rem(flip + lax.rem(t, 2), 2)

    def x_copy(t):
        p = prompt_at(t)
        return pltpu.make_async_copy(
            x_hbm.at[p], gath.at[tp, p], x_sem.at[min(t, early)]
        )

    early = min(2, prompts)
    for t in range(prompts):
        x_copy(t).start()

    barrier = pltpu.get_barrier_semaphore()
    xn = tp + 1 - 2 * lax.rem(tp, 2)
    yn = tp + 2 - 4 * (tp // 2)
    far = n_tp - 1 - tp

    @pl.when(sp > 0)
    def _():
        pl.semaphore_signal(barrier, inc=1, device_id={"sp": sp - 1})

    @pl.when(sp < last)
    def _():
        pl.semaphore_signal(barrier, inc=1, device_id={"sp": sp + 1})

    pl.semaphore_signal(barrier, inc=1, device_id={"tp": xn})
    pl.semaphore_signal(barrier, inc=1, device_id={"tp": yn})
    loads = [
        pltpu.make_async_copy(source, target, local_sem.at[k])
        for k, (source, target) in enumerate(
            (
                (gates_hbm, gates_ref),
                (rate_hbm, rate_ref),
                (bias_hbm, bias_ref),
                (extra_hbm, extra_ref),
                (query_hbm, query_ref),
                (gain_hbm, gain_ref),
                (wk_hbm, w.at[:, pl.ds(0, width)]),
                (wv_hbm, w.at[:, pl.ds(width, nh * DV)]),
            )
        )
    ]
    beside = (sp + last - 1) // last + (2 * last - sp - 1) // last
    pl.semaphore_wait(barrier, 2 + beside)

    half = depth // 2

    def part(at):
        return pl.ds(at * half, half)

    def direct(t, way, first):
        p = prompt_at(t)
        block = gath.at[tp, p, :, part(way if first else 1 - way)]
        return pltpu.make_async_remote_copy(
            src_ref=block,
            dst_ref=block,
            send_sem=gsend.at[0],
            recv_sem=grecv.at[way, t] if first else grecv.at[2, t],
            device_id={"tp": xn if way == 0 else yn},
        )

    def passed(t, way):
        block = gath.at[xn if way == 0 else yn, prompt_at(t), :, part(way)]
        return pltpu.make_async_remote_copy(
            src_ref=block,
            dst_ref=block,
            send_sem=gsend.at[0],
            recv_sem=grecv.at[2, t],
            device_id={"tp": yn if way == 0 else xn},
        )

    def start_direct(t, first):
        for way in range(2):
            direct(t, way, first).start()

    def pass_on(t):
        for way in range(2):
            direct(t, way, True).wait_recv()
            passed(t, way).start()

    def gathered(t):
        blocks = gath.at[pl.ds(0, 2), prompt_at(t)]
        pltpu.make_async_remote_copy(
            src_ref=blocks,
            dst_ref=blocks,
            send_sem=gsend.at[0],
            recv_sem=grecv.at[2, t],
            device_id={"tp": xn},
        ).wait_recv()

    def up_copy(t, full):
        return pltpu.make_async_remote_copy(
            src_ref=up_out.at[t] if full else up_out.at[t, 0],
            dst_ref=up_in.at[t] if full else up_in.at[t, 0],
            send_sem=usend.at[lax.rem(t, 2)],
            recv_sem=urecv.at[t],
            device_id={"sp": sp + 1},
        )

    def down_copy(t, full):
        span = pl.ds(0, down_out.shape[1] if full else low_at)
        return pltpu.make_async_remote_copy(
            src_ref=down_out.at[t, span],
            dst_ref=down_in.at[t, span],
            send_sem=dsend.at[lax.rem(t, 2)],
            recv_sem=drecv.at[t],
            device_id={"sp": sp - 1},
        )

    def on_core(which, act):
        pl.when(core == which)(lambda: act(True))
        pl.when(core != which)(lambda: act(False))

    def read_copy(target, source):
        return pltpu.make_async_remote_copy(
            src_ref=read_buf,
            dst_ref=read_land.at[source],
            send_sem=rsend.at[0],
            recv_sem=rrecv.at[0],
            device_id={"sp": target},
        )

    soon = ((tp, 0), (tp, 1), (xn, 0), (yn, 1))
    late = ((far, 0), (far, 1), (xn, 1), (yn, 0))

    def feature(at):
        return pl.ds(pl.multiple_of(at[0] * depth + at[1] * half, half), half)

    def features(p, which):
        return jnp.concatenate([gath[s, p, :, part(k)] for s, k in which], axis=1)

    def gate_rows(which):
        return jnp.concatenate([gsel[:, feature(at)] for at in which], axis=1)

    def weights(which, cols):
        return jnp.concatenate([w[feature(at), cols] for at in which], axis=0)

    levels = 1
    while (1 << levels) < seg:
        levels += 1
    groups = [(k, min(k + 3, levels)) for k in range(1, levels, 3)]
    tile = DK + DV

    def ahead(t):
        p = prompt_at(t)
        slot = lax.rem(t, 2)
        x = features(p, soon)

        def gate_piece():
            gacc[slot] = dot(gate_rows(soon), x, ((1,), (1,)))

        def piece(at):
            def go():
                cols = pl.ds(at * tile, tile)
                acc[slot, :, cols] = dot(x, weights(soon, cols))

            return go

        return [gate_piece] + [piece(at) for at in range(2 * width // tile)]

    def work(t, pieces):
        pieces = list(pieces)

        def fill():
            if pieces:
                pieces.pop(0)()

        p = prompt_at(t)
        slot = lax.rem(t, 2)
        x = features(p, late)
        gt = gacc[slot] + dot(gate_rows(late), x, ((1,), (1,)))
        key_pre = acc[slot, :, :width] + dot(x, weights(late, pl.ds(0, width)))
        gd = gt[:pad]
        gb = gt[pad:]
        extra = jnp.concatenate([extra_ref[p], jnp.zeros((pad - nh, seg), F32)], axis=0)
        soft = jnp.maximum(gd, 0.0) + jnp.log1p(jnp.exp(-jnp.abs(gd)))
        log_decay = extra - fixed[0] * soft
        beta_pre = gb + fixed[1]
        beta = jax.nn.sigmoid(beta_pre)
        log_beta = jnp.minimum(beta_pre, 0.0) - jnp.log1p(jnp.exp(-jnp.abs(beta_pre)))
        high = log_decay.astype(BF).astype(F32)
        rest = log_decay - high
        mid = rest.astype(BF).astype(F32)
        split = jnp.concatenate([high, mid, rest - mid, jnp.zeros_like(high)], axis=0)
        sums = dot(split.astype(BF), upper[...])
        run = sums[:pad] + sums[pad : 2 * pad] + sums[2 * pad : 3 * pad]
        end = run[:, seg - 1 : seg]
        decs[p] = jnp.broadcast_to(jnp.exp(end), (pad, DV))
        cols = jnp.concatenate(
            [run + log_beta, beta, beta * jnp.exp(run), jnp.exp(end - run)], axis=0
        ).T
        lev = level[...]
        strict = lev >= 0
        hs = range(nh)
        keys, grams = [], []
        for h in hs:
            pre = key_pre[:, h * DK : (h + 1) * DK]
            raw = pre * jax.nn.sigmoid(pre)
            key = raw * lax.rsqrt(jnp.sum(raw * raw, axis=-1, keepdims=True) + EPS)
            kb = key.astype(BF)
            keys.append(key)
            grams.append(dot(kb, kb, ((1,), (1,))))
        value_pre = acc[slot, :, width:] + dot(x, weights(late, pl.ds(width, nh * DV)))
        fill()
        fill()
        sides = []
        for h in hs:
            pre = value_pre[:, h * DV : (h + 1) * DV]
            value = pre * jax.nn.sigmoid(pre)
            spread = cols[:, h : h + 1] - run[h : h + 1, :]
            low = jnp.where(strict, grams[h] * jnp.exp(jnp.where(strict, spread, 0.0)), 0.0)
            cuts = [
                jnp.where(jnp.logical_and(lev >= first, lev < until), low, 0.0)
                for first, until in groups
            ]
            side = [
                value * cols[:, pad + h : pad + h + 1],
                keys[h] * cols[:, 2 * pad + h : 2 * pad + h + 1],
            ]
            whole = jnp.concatenate(cuts + side, axis=1)
            pair = jnp.where(lev == 0, low, 0.0).astype(BF)
            sides.append(whole - dot(pair, whole.astype(BF)))
        fill()
        for first, until in groups:
            steps = [side[:, :seg].astype(BF) for side in sides]
            sides = [side[:, seg:] for side in sides]
            for k in range(first, until):
                final = k == until - 1
                given = [side.astype(BF) for side in sides]
                if not final:
                    given = [jnp.concatenate([e, g], axis=1) for e, g in zip(steps, given)]
                made = [dot(e, g) for e, g in zip(steps, given)]
                if not final:
                    steps = [m[:, :seg].astype(BF) for m in made]
                    made = [m[:, seg:] for m in made]
                sides = [
                    side - m if k == first else side + m for side, m in zip(sides, made)
                ]
                fill()
        while pieces:
            fill()
        tall = ((0,), (0,))
        for h in hs:
            faded = keys[h] * cols[:, 3 * pad + h : 3 * pad + h + 1]
            late_top = faded.astype(BF)
            late_rest = (faded - late_top.astype(F32)).astype(BF)
            top = sides[h].astype(BF)
            rest = (sides[h][:, :DV] - top[:, :DV].astype(F32)).astype(BF)
            both = dot(
                jnp.concatenate([late_top, late_rest], axis=0),
                jnp.concatenate([top, top], axis=0),
                tall,
            )
            adds[p, h] = both[:, :DV] + dot(late_top, rest, tall)
            maps[p, h] = both[:, DV:].astype(BF)

    def moved(at, p, h):
        top = up_in[at, 0, h]
        state = top.astype(F32) + up_in[at, 1, h].astype(F32)
        return decs[p, pl.ds(h, 1)] * state + adds[p, h] - dot(maps[p, h], top)

    def go_up(t, p, fresh):
        for h in range(nh):
            state = adds[p, h] if fresh else moved(t - 1, p, h)
            top = state.astype(BF)
            up_out[t, 0, h] = top
            up_out[t, 1, h] = (state - top.astype(F32)).astype(BF)

    def later(at):
        terms = down_in[at, pl.ds(0, map_at)].astype(F32)
        return terms[:pad] + terms[pad : 2 * pad] + terms[2 * pad : 3 * pad]

    def rows(first, h):
        return pl.ds(first + h * DK, DK)

    def total(at, h):
        top = down_in[at, rows(add_at, h)].astype(F32)
        return top + down_in[at, rows(low_at, h)].astype(F32)

    def go_down(t, p, fresh):
        own = decs[p]
        dec = None if fresh else later(t - 1)
        for h in range(nh):
            add = adds[p, h]
            if fresh:
                down_out[t, rows(map_at, h)] = maps[p, h]
            else:
                above = down_in[t - 1, rows(map_at, h)]
                own_map = maps[p, h]
                turn = dot(above, jnp.concatenate([own_map, add.astype(BF)], axis=1))
                add = dec[h : h + 1] * add + total(t - 1, h) - turn[:, DK:]
                both = dec[h : h + 1] * own_map.astype(F32) + own[h : h + 1] * above.astype(F32)
                down_out[t, rows(map_at, h)] = (both - turn[:, :DK]).astype(BF)
            top = add.astype(BF)
            down_out[t, rows(add_at, h)] = top
            down_out[t, rows(low_at, h)] = (add - top.astype(F32)).astype(BF)
        dec = own if fresh else own * dec
        high = dec.astype(BF).astype(F32)
        rest = dec - high
        mid = rest.astype(BF).astype(F32)
        split = jnp.concatenate([high, mid, rest - mid, jnp.zeros_like(high)], axis=0)
        down_out[t, pl.ds(0, map_at)] = split.astype(BF)

    def wait_up(t):
        on_core(1, lambda full: up_copy(t, full).wait_recv())

    def wait_down(t):
        on_core(0, lambda full: down_copy(t, full).wait_recv())

    def chain_up(t):
        rev = last - t

        @pl.when(sp + rev <= last)
        def _():
            @pl.when(sp == 0)
            def _():
                go_up(t, rev, True)

            @pl.when(sp > 0)
            def _():
                wait_up(t - 1)
                go_up(t, sp + rev, False)

            @pl.when(sp + rev + 2 <= last)
            def _():
                on_core(0, lambda full: up_copy(t - 2, full).wait_send())

            on_core(0, lambda full: up_copy(t, full).start())

    def chain_down(t):
        rev = last - t

        @pl.when(sp >= rev)
        def _():
            @pl.when(sp == last)
            def _():
                go_down(t, last - rev, True)

            @pl.when(sp < last)
            def _():
                wait_down(t - 1)
                go_down(t, sp - rev, False)

            @pl.when(sp >= rev + 2)
            def _():
                on_core(1, lambda full: down_copy(t - 2, full).wait_send())

            on_core(1, lambda full: down_copy(t, full).start())

    def before(t):
        pl.when(core == 0)(lambda: chain_down(t))
        pl.when(core == 1)(lambda: chain_up(t))

    def after(t):
        pl.when(core == 0)(lambda: chain_up(t))
        pl.when(core == 1)(lambda: chain_down(t))

    def close(below, above):
        at = last - 1
        dec = later(at) if above else None
        for h in range(nh):
            state = moved(at, sp, h) if below else adds[sp, h]
            top = state.astype(BF)
            asked = query[h].astype(BF)
            if above:
                turned = dec[h : h + 1] * query[h] - dot(asked, down_in[at, rows(map_at, h)])
                high = turned.astype(BF).astype(F32)
                both = jnp.concatenate([high, turned - high], axis=0).astype(BF)
                terms = dot(both, top)
                raw = (
                    terms[:pad]
                    + terms[pad:]
                    + dot(asked, down_in[at, rows(add_at, h)])
                    + dot(asked, down_in[at, rows(low_at, h)])
                )
            else:
                raw = dot(asked, top)
            norm = (
                raw
                * lax.rsqrt(jnp.mean(raw * raw, axis=-1, keepdims=True) + EPS)
                * gain_ref[...]
            )
            read_buf[pl.ds(h, 1)] = norm[:1]
            if below:
                adds[sp, h] = state

    def store(above):
        at = last - 1
        dec = later(at) if above else None
        for h in range(nh):
            state = adds[sp, h]
            if above:
                state = (
                    dec[h : h + 1] * state
                    + total(at, h)
                    - dot(down_in[at, rows(map_at, h)], state.astype(BF))
                )
            state_out[:, h * DV : (h + 1) * DV] = state.astype(BF)

    for t in range(early):
        x_copy(t).wait()
        start_direct(t, True)
        if t == 0:
            start_direct(t, False)
    for load in loads:
        load.start()
    if early < prompts:
        others = pl.ds(0, prompts - early)
        pltpu.make_async_copy(
            x_hbm.at[others], gath.at[tp, others], x_sem.at[early]
        ).wait()
    for load in loads[:6]:
        load.wait()

    r_id = lax.broadcasted_iota(jnp.int32, (seg, seg), 0)
    c_id = lax.broadcasted_iota(jnp.int32, (seg, seg), 1)
    lev = jnp.zeros((seg, seg), jnp.int32)
    k = 1
    while (1 << k) < seg:
        lev = jnp.where((r_id >> k) != (c_id >> k), k, lev)
        k += 1
    level[...] = jnp.where(r_id > c_id, lev, -1)
    upper[...] = jnp.where(r_id <= c_id, 1.0, 0.0).astype(BF)

    row_id = lax.broadcasted_iota(jnp.int32, (pad, seg), 0)
    rate = jnp.zeros((pad, seg), F32)
    bias = jnp.zeros((pad, seg), F32)
    for h in range(nh):
        rate = jnp.where(row_id == h, rate_ref[h], rate)
        bias = jnp.where(row_id == h, bias_ref[h], bias)
    fixed[0] = rate
    fixed[1] = bias
    for at in range(n_tp * depth // 128):
        chunk = gates_ref[:, at * 128 : (at + 1) * 128].astype(F32)
        gall[at, pl.ds(0, heads)] = chunk[:heads]
        gall[at, pl.ds(heads, heads)] = chunk[heads:]
        gall[at, pl.ds(2 * heads, pad)] = jnp.zeros((pad, 128), F32)
        picked = [gall[at, pl.ds(tp * nh + k * heads, pad)] for k in range(2)]
        gsel[:, at * 128 : (at + 1) * 128] = jnp.concatenate(picked, axis=0).astype(BF)
    every = query_ref[...].astype(F32)
    mine = lax.broadcasted_iota(jnp.int32, every.shape, 0) == sp
    asked = jnp.sum(jnp.where(mine, every, 0.0), axis=0, keepdims=True)
    for h in range(nh):
        query[h] = jnp.broadcast_to(asked[:, h * DK : (h + 1) * DK], (pad, DK))
    read_buf[...] = jnp.zeros_like(read_buf)

    @pl.when(core == 0)
    def _():
        up_in[:, 1] = jnp.zeros((n_sp - 1, nh, DK, DV), BF)

    @pl.when(core == 1)
    def _():
        down_in[:, pl.ds(low_at, nh * DK)] = jnp.zeros((n_sp - 1, nh * DK, DV), BF)


    pass_on(0)
    start_direct(1, False)
    if early < prompts:
        start_direct(early, True)
    for load in loads[6:]:
        load.wait()
    for go in ahead(0):
        go()

    def body(t, carry):
        pass_on(t + 1)

        @pl.when(t + 2 < prompts)
        def _():
            start_direct(t + 2, False)

        @pl.when(t + 3 < prompts)
        def _():
            start_direct(t + 3, True)

        before(t)
        gathered(t)
        work(t, ahead(t + 1))
        after(t)
        return carry

    lax.fori_loop(0, last, body, 0)
    gathered(last)
    work(last, [])

    @pl.when(sp > 0)
    def _():
        wait_up(last - 1)

    @pl.when(sp < last)
    def _():
        wait_down(last - 1)

    @pl.when(sp == 0)
    def _():
        close(False, True)

    @pl.when(jnp.logical_and(sp > 0, sp < last))
    def _():
        close(True, True)

    @pl.when(sp == last)
    def _():
        close(True, False)

    def tell(step, carry):
        target = lax.rem(sp + step, n_sp)
        read_copy(target, sp).start()
        return carry

    lax.fori_loop(1, n_sp, tell, 0)
    read_land[sp] = read_buf[...]
    pl.when(sp < last)(lambda: store(True))
    pl.when(sp == last)(lambda: store(False))

    block = gath.at[pl.ds(0, n_tp - 1)]
    pltpu.make_async_remote_copy(
        src_ref=block,
        dst_ref=block,
        send_sem=gsend.at[0],
        recv_sem=grecv.at[2, 0],
        device_id={"tp": xn},
    ).wait_send()

    for back in range(1, min(last, 2) + 1):

        @pl.when(sp + back <= last)
        def _():
            on_core(0, lambda full: up_copy(last - back, full).wait_send())

        @pl.when(sp >= back)
        def _():
            on_core(1, lambda full: down_copy(last - back, full).wait_send())

    others = read_land.at[pl.ds(0, last)]
    reads = pltpu.make_async_remote_copy(
        src_ref=others,
        dst_ref=others,
        send_sem=rsend.at[0],
        recv_sem=rrecv.at[0],
        device_id={"sp": lax.rem(sp + 1, n_sp)},
    )
    reads.wait_send()
    reads.wait_recv()
    for h in range(nh):
        read_out[:, h * DV : (h + 1) * DV] = read_land[:, h].astype(BF)


def hand_over(state, read, state_out, read_out, sems):
    pairs = ((state, state_out), (read, read_out))
    copies = [pltpu.make_async_copy(a, b, sems.at[k]) for k, (a, b) in enumerate(pairs)]
    for copy in copies:
        copy.start()
    for copy in copies:
        copy.wait()


def close_by(n_sp, n_tp, prompts, seg, depth, rows, nh):
    paired = n_sp >= 4 and n_sp & (n_sp - 1) == 0 and n_tp == 4
    whole = prompts == n_sp and rows == DK and 1 <= nh <= 8
    return paired and whole and seg == 128 and depth % 256 == 0


def shards(
    n_sp,
    n_tp,
    layer_input,
    w_key,
    w_value,
    w_gates,
    decay_rate,
    beta_bias,
    log_decay_extra,
    new_query,
    read_gain,
):
    prompts, seg, depth = layer_input.shape
    whole_depth, width = w_key.shape
    nh = width // DK
    heads = w_gates.shape[2]
    rows = prompts * DK // n_sp
    share = max(nh // 2, 1)
    gates = jnp.swapaxes(w_gates, 1, 2).reshape(2 * heads, whole_depth)
    vmem = pl.BlockSpec(memory_space=pltpu.VMEM)
    smem = pl.BlockSpec(memory_space=pltpu.SMEM)
    hbm = pl.BlockSpec(memory_space=pl.ANY)
    dma = pltpu.SemaphoreType.DMA
    if close_by(n_sp, n_tp, prompts, seg, depth, rows, nh):
        hops = n_sp - 1
        made = pl.pallas_call(
            functools.partial(near, n_sp, n_tp, nh),
            out_shape=(
                pltpu.VMEM((rows, nh * DV), BF),
                pltpu.VMEM((prompts, nh * DV), BF),
            ),
            in_specs=[hbm] * 9,
            out_specs=(vmem, vmem),
            scratch_shapes=[
                pltpu.VMEM((2 * heads, whole_depth), BF),
                pltpu.SMEM((nh,), F32),
                pltpu.SMEM((nh,), F32),
                pltpu.VMEM((prompts, nh, seg), F32),
                pltpu.VMEM((prompts, nh * DK), BF),
                pltpu.VMEM((1, DV), F32),
                pltpu.VMEM((n_tp, prompts, seg, depth), BF),
                pltpu.VMEM((whole_depth, nh * (DK + DV)), BF),
                pltpu.VMEM((whole_depth // 128, 2 * heads + 8, 128), F32),
                pltpu.VMEM((16, whole_depth), BF),
                pltpu.VMEM((2, 8, seg), F32),
                pltpu.VMEM((seg, seg), jnp.int32),
                pltpu.VMEM((seg, seg), BF),
                pltpu.VMEM((2, seg, nh * (DK + DV)), F32),
                pltpu.VMEM((2, 16, seg), F32),
                pltpu.VMEM((prompts, nh, DK, DK), BF),
                pltpu.VMEM((prompts, nh, DK, DV), F32),
                pltpu.VMEM((prompts, 8, DV), F32),
                pltpu.VMEM((hops, 2, nh, DK, DV), BF),
                pltpu.VMEM((hops, 2, nh, DK, DV), BF),
                pltpu.VMEM((hops, 32 + 3 * nh * DK, DV), BF),
                pltpu.VMEM((hops, 32 + 3 * nh * DK, DV), BF),
                pltpu.VMEM((nh, 8, DK), F32),
                pltpu.VMEM((8, DV), F32),
                pltpu.VMEM((prompts, 8, DV), F32),
                dma((8,)),
                dma((min(2, prompts) + 1,)),
                dma((1,)),
                dma((3, prompts)),
                dma((2,)),
                dma((hops,)),
                dma((2,)),
                dma((hops,)),
                dma((1,)),
                dma((1,)),
            ],
            compiler_params=pltpu.CompilerParams(
                collective_id=0, has_side_effects=True, vmem_limit_bytes=56 * 1024 * 1024
            ),
        )(
            layer_input,
            w_key,
            w_value,
            gates,
            decay_rate,
            beta_bias,
            log_decay_extra,
            new_query,
            read_gain.reshape(1, DV),
        )
        return pl.pallas_call(
            hand_over,
            out_shape=tuple(jax.ShapeDtypeStruct(a.shape, a.dtype) for a in made),
            in_specs=[vmem, vmem],
            out_specs=(hbm, hbm),
            scratch_shapes=[dma((2,))],
        )(*[pltpu.with_memory_space_constraint(a, pltpu.VMEM) for a in made])
    return pl.pallas_call(
        functools.partial(kernel, n_sp, n_tp, nh, rows),
        out_shape=(
            jax.ShapeDtypeStruct((rows, nh * DV), BF),
            jax.ShapeDtypeStruct((prompts, nh * DV), BF),
        ),
        in_specs=[hbm, hbm, hbm, vmem, smem, smem, vmem, vmem, vmem],
        out_specs=(vmem, vmem),
        scratch_shapes=[
            pltpu.VMEM((n_tp, prompts, seg, depth), BF),
            pltpu.VMEM((whole_depth, nh * (DK + DV)), BF),
            pltpu.VMEM((2, heads + 8, seg), F32),
            pltpu.VMEM((seg, seg), jnp.int32),
            pltpu.VMEM((seg, seg), F32),
            pltpu.VMEM((prompts, nh, DK, DK), BF),
            pltpu.VMEM((prompts, nh, DK, DV), F32),
            pltpu.VMEM((prompts, 8, DV), F32),
            pltpu.VMEM((prompts, share, DK, DK), BF),
            pltpu.VMEM((prompts, share, DK, DV), F32),
            pltpu.VMEM((prompts, 8, DV), F32),
            pltpu.VMEM((prompts, 8, DV), F32),
            pltpu.VMEM((prompts, share, DK, DV), BF),
            pltpu.VMEM((prompts, share, DK, DV), BF),
            pltpu.VMEM((prompts, share, DK, DV), BF),
            pltpu.VMEM((nh, rows, DV), BF),
            pltpu.VMEM((share, prompts, DV), F32),
            pltpu.VMEM((nh, prompts, DV), F32),
            pltpu.VMEM((nh, prompts, DK), BF),
            dma((3,)),
            dma((max(n_tp, 4), prompts)),
            dma((max(n_tp, 4), prompts)),
            dma((3, prompts)),
            dma((3, prompts)),
            dma((prompts, share)),
            dma((prompts, share)),
            dma((prompts, DK // rows)),
            dma((2,)),
            dma((n_sp,)),
            dma((2,)),
        ],
        compiler_params=pltpu.CompilerParams(
            collective_id=0, has_side_effects=True, vmem_limit_bytes=56 * 1024 * 1024
        ),
    )(
        layer_input,
        w_key,
        w_value,
        gates,
        decay_rate,
        beta_bias,
        log_decay_extra,
        new_query,
        read_gain.reshape(1, DV),
    )


def solution(mesh):
    return jax.shard_map(
        functools.partial(shards, mesh.shape["sp"], mesh.shape["tp"]),
        mesh=mesh,
        in_specs=(
            P(None, "sp", "tp"),
            P(None, "tp"),
            P(None, "tp"),
            P(),
            P("tp"),
            P("tp"),
            P(None, "tp", "sp"),
            P(None, "tp"),
            P(),
        ),
        out_specs=(P("sp", "tp"), P(None, "tp")),
        check_vma=False,
    )
```
